32 devices in a mesh: fs: 4 (over z), rep: 4 (over y, x), tp: 2 (over core).
Axes of the slice: x: 2, y: 2, z: 4, core: 2. Of those that a mesh axis runs over, the one named last changes fastest.
Arguments:
- saved_input: bfloat16 [5632, 2048], P(('fs', 'rep')), may hold values from -6 to 6
- query_cot: bfloat16 [5632, 1024], P(('fs', 'rep'), 'tp'), may hold values from -0.078125 to 0.078125
- attn_out: bfloat16 [5632, 1024], P(('fs', 'rep'), 'tp'), may hold values from -6 to 6
- out_cot: bfloat16 [5632, 2048], P(('fs', 'rep')), may hold values from -0.078125 to 0.078125
- query_basis: bfloat16 [2048, 512], P('fs'), may hold values from -0.25 to 0.25
- output_basis: bfloat16 [2048, 512], P('fs'), may hold values from -0.25 to 0.25
- query_weight: float32 [2048, 1024], P('fs', 'tp'), may hold values from -6 to 6
- output_weight: float32 [1024, 2048], P('tp', 'fs'), may hold values from -6 to 6
- query_moment: float32 [512, 1024], P('rep', 'tp'), may hold values from -52 to 52
- output_moment: float32 [1024, 512], P('tp', 'rep'), may hold values from -52 to 52
Outputs:
- query_step: float32 [2048, 1024], P('fs', 'tp')
- output_step: float32 [1024, 2048], P('tp', 'fs')
- query_new: float32 [2048, 1024], P('fs', 'tp')
- output_new: float32 [1024, 2048], P('tp', 'fs')
- query_copy: bfloat16 [2048, 1024], P('fs', 'tp')
- output_copy: bfloat16 [1024, 2048], P('tp', 'fs')
- query_moment_new: float32 [512, 1024], P('rep', 'tp')
- output_moment_new: float32 [1024, 512], P('tp', 'rep')
The draws below stay inside these ranges and needn't reach their ends.
All inputs are finite; a program needn't handle non-finite values.
Results may differ from the reference program's by a relative error of at most 0.0029.
Values may be sent and summed in bfloat16 or wider, within the bound.
A program may use at most 64 MiB of HBM per device.

```python
import jax
import jax.numpy as jnp
from jax import lax

D = 2048
HEADS = 16
HEAD_DIM = 64
RANK = 512
HD = 1024
TOKENS = 5632


def scaled_field(key, rows, cols):
    first = jax.random.fold_in(key, 11)
    row_pos = jnp.arange(rows, dtype=jnp.float32) / max(rows - 1, 1)
    col_pos = jnp.arange(cols, dtype=jnp.float32) / max(cols - 1, 1)
    base = jnp.clip(jax.random.normal(first, (rows, cols), jnp.float32), -3.0, 3.0)
    row_scale = 1.0 + 3.0 * row_pos
    col_scale = 1.0 + 2.0 * col_pos
    return base * row_scale[:, None] * col_scale[None, :]


def draw_query_moment(key, part):
    return scaled_field(key, RANK, HEADS * HEAD_DIM)


def draw_output_moment(key, part):
    return scaled_field(jax.random.fold_in(key, 5), HEADS * HEAD_DIM, RANK)


def levels(rng, extent, split, low, high):
    gain, own = 1.0, jax.random.fold_in(rng, 6)
    for axis_at, parts in split:
        steps = jnp.exp(jax.random.uniform(jax.random.fold_in(own, axis_at), (parts,), jnp.float32, low / len(split), high / len(split)))
        gain = gain * jnp.repeat(steps, extent[axis_at] // parts).reshape([-1 if axis == axis_at else 1 for axis in range(len(extent))])
    return gain


def scatter_about(rng, extent, scale, bound, split=(), kind=jnp.bfloat16):
    array = scale * jax.random.normal(rng, extent, jnp.float32)
    if split:
        array = array * levels(rng, extent, split, -0.22, 0.18)
    return jnp.clip(array, -bound, bound).astype(kind)


def setup_inputs(seed: int = 0) -> dict:
    splits = jax.random.split(jax.random.key(seed), 11)
    saved_input = scatter_about(splits[0], (TOKENS, D), 1.0, 6.0, ((0, 16),))
    query_cot = scatter_about(splits[1], (TOKENS, HD), (TOKENS ** -0.5), 0.078125, ((0, 16), (1, 2)))
    attn_out = scatter_about(splits[2], (TOKENS, HD), 1.0, 6.0, ((0, 16), (1, 2)))
    out_cot = scatter_about(splits[3], (TOKENS, D), (TOKENS ** -0.5), 0.078125, ((0, 16),))
    query_basis = scatter_about(splits[4], (D, RANK), RANK ** -0.5, 0.25, ((0, 4),))
    output_basis = scatter_about(splits[5], (D, RANK), RANK ** -0.5, 0.25, ((0, 4),))
    query_weight = scatter_about(splits[6], (D, HD), 1.0, 6.0, ((0, 4), (1, 2)), jnp.float32)
    output_weight = scatter_about(splits[7], (HD, D), 1.0, 6.0, ((0, 2), (1, 4)), jnp.float32)
    query_moment = draw_query_moment(jax.random.fold_in(splits[10], 71), 0)
    output_moment = draw_output_moment(jax.random.fold_in(splits[10], 71), 0)
    return dict(saved_input=saved_input, query_cot=query_cot, attn_out=attn_out, out_cot=out_cot, query_basis=query_basis, output_basis=output_basis, query_weight=query_weight, output_weight=output_weight, query_moment=query_moment, output_moment=output_moment)


BETA = 0.8
RATE = 0.2
EPS = 1e-06

def normalize(moment):
    scale = lax.rsqrt(jnp.mean(moment * moment) + EPS)
    return (moment * scale).astype(jnp.bfloat16)

def reference(saved_input, query_cot, attn_out, out_cot, query_basis, output_basis, query_weight, output_weight, query_moment, output_moment):
    query_grad = jnp.dot(saved_input.T, query_cot, preferred_element_type=jnp.float32)
    query_proj = jnp.dot(query_basis.astype(jnp.float32).T, query_grad, precision=lax.Precision.HIGHEST)
    cot_proj = jnp.dot(out_cot, output_basis, preferred_element_type=jnp.float32)
    output_proj = jnp.dot(attn_out.astype(jnp.float32).T, cot_proj, precision=lax.Precision.HIGHEST)
    query_moment_new = BETA * query_moment + (1.0 - BETA) * query_proj
    output_moment_new = BETA * output_moment + (1.0 - BETA) * output_proj
    query_dir = normalize(query_moment_new)
    output_dir = normalize(output_moment_new)
    query_step = jnp.dot(query_basis, query_dir, preferred_element_type=jnp.float32)
    output_step = jnp.dot(output_dir, output_basis.T, preferred_element_type=jnp.float32)
    query_new = query_weight - RATE * query_step
    output_new = output_weight - RATE * output_step
    return (query_step, output_step, query_new, output_new, query_new.astype(jnp.bfloat16), output_new.astype(jnp.bfloat16), query_moment_new, output_moment_new)
```

```python
import functools

import jax
import jax.numpy as jnp
from jax import lax
from jax.experimental import pallas as pl
from jax.experimental.pallas import tpu as pltpu
from jax.sharding import PartitionSpec as P

BETA = 0.8
RATE = 0.2
EPS = 1e-06


def on_device(
    saved_input,
    query_cot,
    attn_out,
    out_cot,
    query_basis,
    output_basis,
    query_weight,
    output_weight,
    query_moment,
    output_moment,
):
    rank = query_basis.shape[1]
    grad_rows = lax.psum_scatter(
        jnp.dot(saved_input.T, query_cot, preferred_element_type=jnp.float32),
        "fs",
        scatter_dimension=0,
        tiled=True,
    )
    query_part = jnp.dot(
        query_basis.astype(jnp.float32).T, grad_rows, precision=lax.Precision.HIGHEST
    )
    cot_proj = jnp.dot(
        out_cot,
        lax.all_gather(output_basis, "fs", axis=0, tiled=True),
        preferred_element_type=jnp.float32,
    )
    output_part = jnp.dot(attn_out.astype(jnp.float32).T, cot_proj, precision=lax.Precision.HIGHEST)
    reps = lax.axis_size("rep")
    share = rank // reps
    query_terms, output_terms = (
        lax.all_to_all(
            query_part.astype(jnp.bfloat16), "rep", split_axis=0, concat_axis=0, tiled=True
        ).astype(query_part.dtype),
        lax.all_to_all(
            output_part.T.astype(jnp.bfloat16), "rep", split_axis=0, concat_axis=0, tiled=True
        ).astype(jnp.float32),
    )
    width = query_part.shape[1]
    query_local = jnp.sum(query_terms.reshape(reps, share, width), axis=0)
    output_local = jnp.sum(output_terms.reshape(reps, share, width), axis=0)
    query_share, output_flip = lax.psum((query_local, output_local), "fs")
    output_share = output_flip.T
    query_moment_new = BETA * query_moment + (1.0 - BETA) * query_share
    output_moment_new = BETA * output_moment + (1.0 - BETA) * output_share
    query_squares, output_squares = lax.psum(
        (
            jnp.sum(query_moment_new * query_moment_new),
            jnp.sum(output_moment_new * output_moment_new),
        ),
        ("rep", "tp"),
    )
    entries = rank * query_moment.shape[1] * lax.axis_size("tp")
    query_dir = (query_moment_new * lax.rsqrt(query_squares / entries + EPS)).astype(jnp.bfloat16)
    output_dir = (output_moment_new * lax.rsqrt(output_squares / entries + EPS)).astype(
        jnp.bfloat16
    )
    query_full, output_full = (
        lax.all_gather(query_dir, "rep", axis=0, tiled=True),
        lax.all_gather(output_dir, "rep", axis=1, tiled=True),
    )
    query_step = jnp.dot(query_basis, query_full, preferred_element_type=jnp.float32)
    output_step = jnp.dot(output_full, output_basis.T, preferred_element_type=jnp.float32)
    query_new = query_weight - RATE * query_step
    output_new = output_weight - RATE * output_step
    return (
        query_step,
        output_step,
        query_new,
        output_new,
        query_new.astype(jnp.bfloat16),
        output_new.astype(jnp.bfloat16),
        query_moment_new,
        output_moment_new,
    )


MESH = pl.DeviceIdType.MESH
UNITS = 4


def exchange_kernel(
    si_hbm, oc_hbm, qc_hbm, ao_hbm, qb_hbm, ob_hbm, mq_hbm, mo_hbm,
    full_out, mom_out, norm_out,
    act, cot, base, old, mo, gath, pb, t1, sb, t2, ag, mom, nrm, full, total_sq,
    load_sem, store_sem, cx_s, cx_r, az_s, az_r, aw_s, aw_r,
    b1_s, b1_r, b2_s, b2_r, g_s, g_r, n_s, n_r, d_s, d_r,
):
    f, r, t = lax.axis_index("fs"), lax.axis_index("rep"), lax.axis_index("tp")
    y, x = r // 2, r % 2
    ot = 1 - t
    fpeer = [(f + d) % 4 for d in (1, 3, 2)]
    fsrc = [(f + 4 - d) % 4 for d in (1, 3, 2)]
    rpeer = [2 * y + (1 - x), 2 * (1 - y) + x, 3 - r]
    depth, half = base.shape[1], base.shape[2]
    hd = depth // 2
    share = half // 2
    cut = share // 2
    piece = cut // 4

    cols = pl.ds(pl.multiple_of(t * half, half), half)
    loads = []
    for k, (src, dst) in enumerate((
        (qb_hbm.at[:, cols], base.at[0]), (ob_hbm.at[:, cols], base.at[1]),
        (qc_hbm, cot.at[0, t]), (ao_hbm, cot.at[1, t]),
        (si_hbm, act.at[0]), (oc_hbm, act.at[1]),
        (mq_hbm, old.at[0]), (mo_hbm, mo),
    )):
        c = pltpu.make_async_copy(src, dst, load_sem.at[k])
        c.start()
        loads.append(c)

    barrier = pltpu.get_barrier_semaphore()
    for g in fpeer:
        pl.semaphore_signal(barrier, inc=1, device_id=(g, r, t), device_id_type=MESH)
    for q in rpeer:
        for s in (t, ot):
            pl.semaphore_signal(barrier, inc=1, device_id=(f, q, s), device_id_type=MESH)
    pl.semaphore_signal(barrier, inc=1, device_id=(f, r, ot), device_id_type=MESH)

    for p in range(2):
        loads[p].wait()
        lo, hi = base[p, :, :share], base[p, :, share:]
        gath[2 * p, f] = jnp.concatenate([lo[:, :cut], hi[:, :cut]], axis=1)
        gath[2 * p + 1, f] = jnp.concatenate([lo[:, cut:], hi[:, cut:]], axis=1)

    pl.semaphore_wait(barrier, 10)

    def remote(src, dst, ss, rs, dev):
        return pltpu.make_async_remote_copy(
            src_ref=src, dst_ref=dst, send_sem=ss, recv_sem=rs, device_id=dev, device_id_type=MESH
        )

    h = x * (1 - t) + y * t
    near = rpeer[0] * (1 - t) + rpeer[1] * t
    mine = pl.ds(pl.multiple_of(h * hd, hd), hd)
    theirs = pl.ds(pl.multiple_of((1 - h) * hd, hd), hd)
    last = 3

    def line(u, way, s, arrive=False):
        step = -1 if way == 0 else 1
        slab = f + step * s + (step if arrive else 0)
        ref = gath.at[u, slab, mine, :]
        dev = f + step if arrive else f - step
        return remote(ref, ref, az_s.at[u, way, s], az_r.at[u, way, s], (dev, r, t))

    def sends_line(way, s):
        return (f >= s) & (f < last) if way == 0 else (f + s <= last) & (f > 0)

    def gets_line(way, s):
        return f >= s + 1 if way == 0 else f + s + 1 <= last

    def carried(way):
        return f if way == 0 else last - f

    def share_slab(u, slab, rows):
        ref = gath.at[u, slab, rows, :]
        return remote(ref, ref, aw_s.at[u, slab], aw_r.at[u, slab], (f, near, t))

    def open_line(u, count=None):
        for way in range(2):
            go = sends_line(way, 0)
            if count is not None:
                go = go & (carried(way) == count)

            @pl.when(go)
            def _():
                line(u, way, 0).start()

    def run_line(u, s):
        for way in range(2):
            @pl.when(gets_line(way, s))
            def _():
                line(u, way, s, True).wait_recv()
            if s < 2:
                @pl.when(sends_line(way, s + 1))
                def _():
                    line(u, way, s + 1).start()

            @pl.when(gets_line(way, s))
            def _():
                slab = f - 1 - s if way == 0 else f + 1 + s
                share_slab(u, slab, mine).start()

    def swap_cot(p):
        ref = cot.at[p, t]
        return remote(ref, ref, cx_s.at[p], cx_r.at[p], (f, r, ot))

    def got_cot(p):
        ref = cot.at[p, ot]
        return remote(ref, ref, cx_s.at[p], cx_r.at[p], (f, r, ot))

    def to_reps(u, k):
        j = 1 - x if k < 2 else x
        c = (0, 1, ot, t)[k]
        return remote(
            pb.at[u, j, c], t1.at[u, r], b1_s.at[u, k], b1_r.at[u, r], (f, 2 * t + j, c)
        )

    def from_rep(u, q):
        return remote(t1.at[u, q], t1.at[u, q], b1_s.at[u, 0], b1_r.at[u, q], (f, q, y))

    def scatter_reps(u):
        p = u // 2
        for g in fsrc:
            share_slab(u, g, theirs).wait_recv()
        part = jnp.dot(act[p, :, :depth], gath[u, 0], preferred_element_type=jnp.float32)
        for g in range(1, 4):
            part = part + jnp.dot(
                act[p, :, g * depth : (g + 1) * depth], gath[u, g],
                preferred_element_type=jnp.float32,
            )
        part = part.astype(jnp.bfloat16)
        for c in range(2):
            terms = lax.dot_general(
                part, cot[p, c], (((0,), (0,)), ((), ())), preferred_element_type=jnp.float32
            )
            for j in range(2):
                pb[u, j, c] = terms[j * cut : (j + 1) * cut].astype(jnp.bfloat16)
        for k in range(3):
            to_reps(u, k).start()

        @pl.when(t != y)
        def _():
            to_reps(u, 3).start()

        @pl.when(t == y)
        def _():
            t1[u, r] = pb[u, x, t]

    def scatter_tokens(u):
        for q in (rpeer[0], rpeer[1], rpeer[2]):
            from_rep(u, q).wait_recv()

        @pl.when(t != y)
        def _():
            from_rep(u, r).wait_recv()

        total = t1[u, 0].astype(jnp.float32)
        for q in range(1, 4):
            total = total + t1[u, q].astype(jnp.float32)
        for g in range(4):
            sb[u, g] = total[g * piece : (g + 1) * piece].astype(jnp.bfloat16)
        for k in (2, 0, 1):
            to_token(u, k).start()

    def to_token(u, k):
        return remote(
            sb.at[u, fpeer[k]], t2.at[u, k], b2_s.at[u, k], b2_r.at[u, k], (fpeer[k], r, t)
        )

    def rows_at(u, g):
        at = (u % 2) * cut + g * piece
        return pl.ds(pl.multiple_of(at, piece), piece)

    def to_dirs(u, g, k):
        ref = full.at[u // 2, r, rows_at(u, g), :]
        return remote(ref, ref, d_s.at[u, g, k], d_r.at[u, g, k], (f, rpeer[k], t))

    def got_dirs(u, g, k):
        ref = full.at[u // 2, rpeer[k], rows_at(u, g), :]
        return remote(ref, ref, d_s.at[u, g, k], d_r.at[u, g, k], (f, rpeer[k], t))

    def to_sums(u, k):
        return remote(
            ag.at[u, f], ag.at[u, f], g_s.at[u, k], g_r.at[u, k], (fpeer[k], r, t)
        )

    def got_sums(u, k):
        ref = ag.at[u, fsrc[k]]
        return remote(ref, ref, g_s.at[u, k], g_r.at[u, k], (fsrc[k], r, t))

    def update(u, g):
        p, rows = u // 2, rows_at(u, g)
        new = BETA * old[p, rows, :] + (1.0 - BETA) * ag[u, g].astype(jnp.float32)
        mom[p, rows, :] = new
        full[p, r, rows, :] = new.astype(jnp.bfloat16)
        for k in (2, 0, 1):
            to_dirs(u, g, k).start()

    def gather_sums(u):
        total = sb[u, f].astype(jnp.float32)
        for k in range(3):
            to_token(u, k).wait_recv()
            total = total + t2[u, k].astype(jnp.float32)
        ag[u, f] = total.astype(jnp.bfloat16)
        for k in (2, 0, 1):
            to_sums(u, k).start()
        update(u, f)

    def gather_dirs(u):
        for k in range(3):
            got_sums(u, k).wait_recv()
            update(u, fsrc[k])

    others = [(q, s) for q in rpeer for s in (t, ot)] + [(r, ot)]
    me = 2 * r + t

    def to_norms(p, k):
        q, s = others[k]
        ref = nrm.at[p, me]
        return remote(ref, ref, n_s.at[p, k], n_r.at[p, k], (f, q, s))

    def got_norms(p, k):
        q, s = others[k]
        ref = nrm.at[p, 2 * q + s]
        return remote(ref, ref, n_s.at[p, k], n_r.at[p, k], (f, q, s))

    def send_norms(p):
        sq = mom[p] * mom[p]
        lanes = sq[:, :128]
        for k in range(1, sq.shape[1] // 128):
            lanes = lanes + sq[:, k * 128 : (k + 1) * 128]
        acc = lanes[:8]
        for k in range(1, share // 8):
            acc = acc + lanes[k * 8 : (k + 1) * 8]
        nrm[p, me] = acc
        for k in range(7):
            to_norms(p, k).start()

    def sum_norms(p):
        for k in range(7):
            got_norms(p, k).wait_recv()
        acc = nrm[p, 0]
        for k in range(1, 8):
            acc = acc + nrm[p, k]
        total_sq[p] = acc

    def stores(p):
        return [
            pltpu.make_async_copy(full.at[p], full_out.at[p], store_sem.at[p, 0]),
            pltpu.make_async_copy(mom.at[p], mom_out.at[p], store_sem.at[p, 1]),
            pltpu.make_async_copy(total_sq.at[p], norm_out.at[p], store_sem.at[p, 2]),
        ]

    def finish(p):
        stores(p)[1].start()
        sum_norms(p)
        stores(p)[2].start()
        for u in (2 * p, 2 * p + 1):
            for g in [f] + fsrc:
                for k in range(3):
                    got_dirs(u, g, k).wait_recv()
        stores(p)[0].start()

    open_line(0)
    open_line(1)
    open_line(2, 0)
    open_line(3, 0)
    for p in range(2):
        loads[2 + p].wait()
        swap_cot(p).start()
    loads[6].wait()
    loads[7].wait()
    old[1] = mo[...].T
    run_line(0, 0)
    run_line(1, 0)
    open_line(2, 1)
    run_line(0, 1)
    run_line(1, 1)
    open_line(2, 2)
    run_line(2, 0)
    open_line(3, 1)
    run_line(0, 2)
    run_line(1, 2)
    loads[4].wait()
    got_cot(0).wait_recv()
    scatter_reps(0)
    run_line(2, 1)
    open_line(3, 2)
    scatter_reps(1)
    run_line(3, 0)
    run_line(2, 2)
    run_line(3, 1)
    loads[5].wait()
    got_cot(1).wait_recv()
    scatter_reps(2)
    run_line(3, 2)
    scatter_tokens(0)
    scatter_reps(3)
    scatter_tokens(1)
    gather_sums(0)
    scatter_tokens(2)
    gather_sums(1)
    scatter_tokens(3)
    gather_dirs(0)
    gather_sums(2)
    gather_dirs(1)
    send_norms(0)
    gather_sums(3)
    gather_dirs(2)
    gather_dirs(3)
    send_norms(1)
    finish(0)
    finish(1)
    for u in range(UNITS):
        for way in range(2):
            for s in range(3):
                @pl.when(sends_line(way, s))
                def _():
                    line(u, way, s).wait_send()
        for k in range(3):
            share_slab(u, fsrc[k], mine).wait_send()
            to_reps(u, k).wait_send()
            to_token(u, k).wait_send()
            to_sums(u, k).wait_send()
            for g in range(4):
                to_dirs(u, g, k).wait_send()

        @pl.when(t != y)
        def _():
            to_reps(u, 3).wait_send()

    for p in range(2):
        swap_cot(p).wait_send()
        for k in range(7):
            to_norms(p, k).wait_send()
        for c in stores(p):
            c.wait()


def finish_kernel(
    entries, qb, ob, fq, fo, sq, qw, ow, mq, mo,
    qs_o, os_o, qn_o, on_o, qc_o, oc_o, mq_o, mo_o,
):
    def scale(p):
        rows = jnp.sum(sq[p], axis=0, keepdims=True)
        return lax.rsqrt(jnp.sum(rows, axis=1, keepdims=True) / entries + EPS)

    step = jnp.dot(qb[...], fq[0], preferred_element_type=jnp.float32) * scale(0)
    new = qw[...] - RATE * step
    qs_o[...] = step
    qn_o[...] = new
    qc_o[...] = new.astype(jnp.bfloat16)
    step = lax.dot_general(
        fo[0].T, ob[...], (((1,), (1,)), ((), ())), preferred_element_type=jnp.float32
    ) * scale(1)
    new = ow[...] - RATE * step
    os_o[...] = step
    on_o[...] = new
    oc_o[...] = new.astype(jnp.bfloat16)
    mq_o[...] = mq[0]
    mo_o[...] = mo[0].T


def on_device_fast(
    saved_input, query_cot, attn_out, out_cot, query_basis, output_basis,
    query_weight, output_weight, query_moment, output_moment,
):
    tokens, depth_all = saved_input.shape
    width = query_cot.shape[1]
    depth, rank = query_basis.shape
    share = rank // 4
    cut = share // 2
    piece = cut // 4
    entries = rank * width * lax.axis_size("tp")
    bf, f32 = jnp.bfloat16, jnp.float32
    any_spec = pl.BlockSpec(memory_space=pl.ANY)
    dma = pltpu.SemaphoreType.DMA
    ins = (
        saved_input, out_cot, query_cot, attn_out, query_basis, output_basis,
        query_moment, output_moment,
    )
    full, mom, norm = pl.pallas_call(
        exchange_kernel,
        out_shape=(
            jax.ShapeDtypeStruct((2, 4, share, width), bf),
            jax.ShapeDtypeStruct((2, share, width), f32),
            jax.ShapeDtypeStruct((2, 8, 128), f32),
        ),
        in_specs=[any_spec] * 8,
        out_specs=(any_spec, any_spec, any_spec),
        scratch_shapes=[
            pltpu.VMEM((2, tokens, depth_all), bf),
            pltpu.VMEM((2, 2, tokens, width), bf),
            pltpu.VMEM((2, depth, rank // 2), bf),
            pltpu.VMEM((2, share, width), f32),
            pltpu.VMEM((width, share), f32),
            pltpu.VMEM((UNITS, 4, depth, share), bf),
            pltpu.VMEM((UNITS, 2, 2, cut, width), bf),
            pltpu.VMEM((UNITS, 4, cut, width), bf),
            pltpu.VMEM((UNITS, 4, piece, width), bf),
            pltpu.VMEM((UNITS, 3, piece, width), bf),
            pltpu.VMEM((UNITS, 4, piece, width), bf),
            pltpu.VMEM((2, share, width), f32),
            pltpu.VMEM((2, 8, 8, 128), f32),
            pltpu.VMEM((2, 4, share, width), bf),
            pltpu.VMEM((2, 8, 128), f32),
            dma((8,)), dma((2, 3)), dma((2,)), dma((2,)),
            dma((UNITS, 2, 3)), dma((UNITS, 2, 3)), dma((UNITS, 4)), dma((UNITS, 4)),
            dma((UNITS, 4)), dma((UNITS, 4)), dma((UNITS, 3)), dma((UNITS, 3)),
            dma((UNITS, 3)), dma((UNITS, 3)), dma((2, 7)), dma((2, 7)),
            dma((UNITS, 4, 3)), dma((UNITS, 4, 3)),
        ],
        compiler_params=pltpu.CompilerParams(
            collective_id=0, has_side_effects=True, vmem_limit_bytes=20 * 2**20
        ),
    )(*(pltpu.with_memory_space_constraint(a, pltpu.HBM) for a in ins))
    full = full.reshape(2, rank, width)
    n = 4
    rows = pl.BlockSpec((depth // n, rank), lambda i: (i, 0))
    whole = pl.BlockSpec((depth, rank), lambda i: (0, 0))
    wq = pl.BlockSpec((depth // n, width), lambda i: (i, 0))
    wo = pl.BlockSpec((width // n, depth), lambda i: (i, 0))
    mq = pl.BlockSpec((share // n, width), lambda i: (i, 0))
    mo = pl.BlockSpec((width // n, share), lambda i: (i, 0))
    sq, so = query_weight.shape, output_weight.shape
    return pl.pallas_call(
        functools.partial(finish_kernel, entries),
        grid=(n,),
        out_shape=tuple(
            jax.ShapeDtypeStruct(s, d)
            for s, d in (
                (sq, f32), (so, f32), (sq, f32), (so, f32), (sq, bf), (so, bf),
                (query_moment.shape, f32), (output_moment.shape, f32),
            )
        ),
        in_specs=[
            rows, whole,
            pl.BlockSpec((1, rank, width), lambda i: (0, 0, 0)),
            pl.BlockSpec((1, rank, width // n), lambda i: (1, 0, i)),
            pl.BlockSpec((2, 8, 128), lambda i: (0, 0, 0)),
            wq, wo,
            pl.BlockSpec((1, share // n, width), lambda i: (0, i, 0)),
            pl.BlockSpec((1, share, width // n), lambda i: (1, 0, i)),
        ],
        out_specs=(wq, wo, wq, wo, wq, wo, mq, mo),
        cost_estimate=pl.CostEstimate(
            flops=4 * depth * rank * width, bytes_accessed=20 * depth * width, transcendentals=0
        ),
        compiler_params=pltpu.CompilerParams(vmem_limit_bytes=20 * 2**20),
    )(query_basis, output_basis, full, full, norm, query_weight, output_weight, mom, mom)


def solution(mesh):
    small = dict(mesh.shape) == {"fs": 4, "rep": 4, "tp": 2}
    body = on_device_fast if small else on_device
    placed = (
        P(("fs", "rep"), None),
        P(("fs", "rep"), "tp"),
        P(("fs", "rep"), "tp"),
        P(("fs", "rep"), None),
        P("fs", None),
        P("fs", None),
        P("fs", "tp"),
        P("tp", "fs"),
        P("rep", "tp"),
        P("tp", "rep"),
    )
    return jax.shard_map(
        body,
        mesh=mesh,
        in_specs=placed,
        out_specs=(
            P("fs", "tp"),
            P("tp", "fs"),
            P("fs", "tp"),
            P("tp", "fs"),
            P("fs", "tp"),
            P("tp", "fs"),
            P("rep", "tp"),
            P("tp", "rep"),
        ),
        check_vma=False,
    )
```

```python
import functools

import jax
import jax.numpy as jnp
from jax import lax
from jax.experimental import pallas as pl
from jax.experimental.pallas import tpu as pltpu
from jax.sharding import PartitionSpec as P

BETA = 0.8
RATE = 0.2
EPS = 1e-06


def on_device(
    saved_input,
    query_cot,
    attn_out,
    out_cot,
    query_basis,
    output_basis,
    query_weight,
    output_weight,
    query_moment,
    output_moment,
):
    rank = query_basis.shape[1]
    grad_rows = lax.psum_scatter(
        jnp.dot(saved_input.T, query_cot, preferred_element_type=jnp.float32),
        "fs",
        scatter_dimension=0,
        tiled=True,
    )
    query_part = jnp.dot(
        query_basis.astype(jnp.float32).T, grad_rows, precision=lax.Precision.HIGHEST
    )
    cot_proj = jnp.dot(
        out_cot,
        lax.all_gather(output_basis, "fs", axis=0, tiled=True),
        preferred_element_type=jnp.float32,
    )
    output_part = jnp.dot(attn_out.astype(jnp.float32).T, cot_proj, precision=lax.Precision.HIGHEST)
    reps = lax.axis_size("rep")
    share = rank // reps
    query_terms, output_terms = (
        lax.all_to_all(
            query_part.astype(jnp.bfloat16), "rep", split_axis=0, concat_axis=0, tiled=True
        ).astype(query_part.dtype),
        lax.all_to_all(
            output_part.T.astype(jnp.bfloat16), "rep", split_axis=0, concat_axis=0, tiled=True
        ).astype(jnp.float32),
    )
    width = query_part.shape[1]
    query_local = jnp.sum(query_terms.reshape(reps, share, width), axis=0)
    output_local = jnp.sum(output_terms.reshape(reps, share, width), axis=0)
    query_share, output_flip = lax.psum((query_local, output_local), "fs")
    output_share = output_flip.T
    query_moment_new = BETA * query_moment + (1.0 - BETA) * query_share
    output_moment_new = BETA * output_moment + (1.0 - BETA) * output_share
    query_squares, output_squares = lax.psum(
        (
            jnp.sum(query_moment_new * query_moment_new),
            jnp.sum(output_moment_new * output_moment_new),
        ),
        ("rep", "tp"),
    )
    entries = rank * query_moment.shape[1] * lax.axis_size("tp")
    query_dir = (query_moment_new * lax.rsqrt(query_squares / entries + EPS)).astype(jnp.bfloat16)
    output_dir = (output_moment_new * lax.rsqrt(output_squares / entries + EPS)).astype(
        jnp.bfloat16
    )
    query_full, output_full = (
        lax.all_gather(query_dir, "rep", axis=0, tiled=True),
        lax.all_gather(output_dir, "rep", axis=1, tiled=True),
    )
    query_step = jnp.dot(query_basis, query_full, preferred_element_type=jnp.float32)
    output_step = jnp.dot(output_full, output_basis.T, preferred_element_type=jnp.float32)
    query_new = query_weight - RATE * query_step
    output_new = output_weight - RATE * output_step
    return (
        query_step,
        output_step,
        query_new,
        output_new,
        query_new.astype(jnp.bfloat16),
        output_new.astype(jnp.bfloat16),
        query_moment_new,
        output_moment_new,
    )


MESH = pl.DeviceIdType.MESH
UNITS = 4


def exchange_kernel(
    si_hbm, oc_hbm, qc_hbm, ao_hbm, qb_hbm, ob_hbm, mq_hbm, mo_hbm,
    full, mom, total_sq,
    act, cot, base, old, mo, gath, own, pb, t1, sb, t2, ag, nrm,
    load_sem, sent, cx_r, az_r, aw_r, b1_r, b2_r, g_r, n_r, d_r,
):
    f, r, t = lax.axis_index("fs"), lax.axis_index("rep"), lax.axis_index("tp")
    y, x = r // 2, r % 2
    ot = 1 - t
    fpeer = [(f + d) % 4 for d in (1, 3, 2)]
    fsrc = [(f + 4 - d) % 4 for d in (1, 3, 2)]
    rpeer = [2 * y + (1 - x), 2 * (1 - y) + x, 3 - r]
    depth, half = base.shape[1], base.shape[2]
    hd = depth // 2
    share = half // 2
    cut = share // 2
    piece = cut // 4

    cols = pl.ds(pl.multiple_of(t * half, half), half)
    loads = []
    for k, (src, dst) in enumerate((
        (qb_hbm.at[:, cols], base.at[0]), (ob_hbm.at[:, cols], base.at[1]),
        (qc_hbm, cot.at[0, t]), (ao_hbm, cot.at[1, t]),
        (si_hbm, act.at[0]), (oc_hbm, act.at[1]),
        (mq_hbm, old.at[0]), (mo_hbm, mo),
    )):
        c = pltpu.make_async_copy(src, dst, load_sem.at[k])
        c.start()
        loads.append(c)

    barrier = pltpu.get_barrier_semaphore()
    for g in fpeer:
        pl.semaphore_signal(barrier, inc=1, device_id=(g, r, t), device_id_type=MESH)
    for q in rpeer:
        for s in (t, ot):
            pl.semaphore_signal(barrier, inc=1, device_id=(f, q, s), device_id_type=MESH)
    pl.semaphore_signal(barrier, inc=1, device_id=(f, r, ot), device_id_type=MESH)

    for p in range(2):
        loads[p].wait()
        lo, hi = base[p, :, :share], base[p, :, share:]
        gath[p, f, :, :share] = jnp.concatenate([lo[:, :cut], hi[:, :cut]], axis=1)
        gath[p, f, :, share:] = jnp.concatenate([lo[:, cut:], hi[:, cut:]], axis=1)

    pl.semaphore_wait(barrier, 10)

    def remote(src, dst, ss, rs, dev):
        return pltpu.make_async_remote_copy(
            src_ref=src, dst_ref=dst, send_sem=ss, recv_sem=rs, device_id=dev, device_id_type=MESH
        )

    def settle(ref, sem):
        pltpu.make_async_copy(ref, ref, sem).wait()

    h = x * (1 - t) + y * t
    near = rpeer[0] * (1 - t) + rpeer[1] * t
    mine = pl.ds(pl.multiple_of(h * hd, hd), hd)
    theirs = pl.ds(pl.multiple_of((1 - h) * hd, hd), hd)
    last = 3

    def unit_ref(u, slab, rows):
        k = u % 2
        return gath.at[u // 2, slab, rows, k * share : (k + 1) * share]

    def line(u, way, s, arrive=False):
        step = -1 if way == 0 else 1
        slab = f + step * s + (step if arrive else 0)
        ref = unit_ref(u, slab, mine)
        dev = f + step if arrive else f - step
        to = f if arrive else dev
        slot = s if way == 0 else to + s
        return remote(ref, ref, sent.at[min(s, 1)], az_r.at[u, slot], (dev, r, t))

    def sends_line(way, s):
        return (f >= s) & (f < last) if way == 0 else (f + s <= last) & (f > 0)

    def gets_line(way, s):
        return f >= s + 1 if way == 0 else f + s + 1 <= last

    def carried(way):
        return f if way == 0 else last - f

    def share_slab(u, slab, rows):
        ref = unit_ref(u, slab, rows)
        return remote(ref, ref, sent.at[2], aw_r.at[u], (f, near, t))

    def open_line(u, count=None):
        for way in range(2):
            go = sends_line(way, 0)
            if count is not None:
                go = go & (carried(way) == count)

            @pl.when(go)
            def _():
                line(u, way, 0).start()

    def run_line(u, s):
        for way in range(2):
            @pl.when(gets_line(way, s))
            def _():
                line(u, way, s, True).wait_recv()
            if s < 2:
                @pl.when(sends_line(way, s + 1))
                def _():
                    line(u, way, s + 1).start()

            @pl.when(gets_line(way, s))
            def _():
                slab = f - 1 - s if way == 0 else f + 1 + s
                share_slab(u, slab, mine).start()

    def swap_cot(p):
        ref = cot.at[p, t]
        return remote(ref, ref, sent.at[3], cx_r.at[p], (f, r, ot))

    def to_reps(u, k):
        j = 1 - x if k < 2 else x
        c = (0, 1, ot, t)[k]
        return remote(
            pb.at[u, j, c], t1.at[u, r], sent.at[4], b1_r.at[u], (f, 2 * t + j, c)
        )

    def slab_dot(p, g, lanes):
        at = pl.ds(pl.multiple_of(g * depth, depth), depth)
        return jnp.dot(act[p, :, at], gath[p, g, :, lanes], preferred_element_type=jnp.float32)

    def project(p, us):
        for u in us:
            k = u % 2
            settle(gath.at[p, :3, theirs, k * share : (k + 1) * share], aw_r.at[u])
        lanes = slice((us[0] % 2) * share, (us[-1] % 2 + 1) * share)
        part = own[p, :, lanes]
        for g in fsrc:
            part = part + slab_dot(p, g, lanes)
        part = part.astype(jnp.bfloat16)
        for c in range(2):
            terms = lax.dot_general(
                part, cot[p, c], (((0,), (0,)), ((), ())), preferred_element_type=jnp.float32
            )
            for i, u in enumerate(us):
                for j in range(2):
                    at = i * share + j * cut
                    pb[u, j, c] = terms[at : at + cut].astype(jnp.bfloat16)

    def scatter_reps(u):
        for k in range(3):
            to_reps(u, k).start()

        @pl.when(t != y)
        def _():
            to_reps(u, 3).start()

        @pl.when(t == y)
        def _():
            t1[u, r] = pb[u, x, t]

    def scatter_tokens(u):
        @pl.when(t != y)
        def _():
            settle(t1.at[u], b1_r.at[u])

        @pl.when(t == y)
        def _():
            settle(t1.at[u, :3], b1_r.at[u])

        total = t1[u, 0].astype(jnp.float32)
        for q in range(1, 4):
            total = total + t1[u, q].astype(jnp.float32)
        for g in range(4):
            sb[u, g] = total[g * piece : (g + 1) * piece].astype(jnp.bfloat16)
        for k in (2, 0, 1):
            to_token(u, k).start()

    def to_token(u, k):
        return remote(
            sb.at[u, fpeer[k]], t2.at[u, k], sent.at[5], b2_r.at[u], (fpeer[k], r, t)
        )

    def rows_at(u, g):
        at = (u % 2) * cut + g * piece
        return pl.ds(pl.multiple_of(at, piece), piece)

    def to_dirs(u, g, k):
        ref = full.at[u // 2, r, rows_at(u, g), :]
        return remote(ref, ref, sent.at[7], d_r.at[u // 2], (f, rpeer[k], t))

    def to_sums(u, k):
        return remote(
            ag.at[u, f], ag.at[u, f], sent.at[6], g_r.at[u, k], (fpeer[k], r, t)
        )

    def update(u, g):
        p, rows = u // 2, rows_at(u, g)
        new = BETA * old[p, rows, :] + (1.0 - BETA) * ag[u, g].astype(jnp.float32)
        mom[p, rows, :] = new
        full[p, r, rows, :] = new.astype(jnp.bfloat16)
        for k in (2, 0, 1):
            to_dirs(u, g, k).start()

    def gather_sums(u):
        total = sb[u, f].astype(jnp.float32)
        settle(t2.at[u], b2_r.at[u])
        for k in range(3):
            total = total + t2[u, k].astype(jnp.float32)
        ag[u, f] = total.astype(jnp.bfloat16)
        for k in (2, 0, 1):
            to_sums(u, k).start()
        update(u, f)

    def gather_dirs(u):
        for k in range(3):
            settle(ag.at[u, fsrc[k]], g_r.at[u, k])
            update(u, fsrc[k])

    others = [(q, s) for q in rpeer for s in (t, ot)] + [(r, ot)]
    me = 2 * r + t

    def to_norms(p, k):
        q, s = others[k]
        ref = nrm.at[p, me]
        return remote(ref, ref, sent.at[8], n_r.at[p], (f, q, s))

    def send_norms(p):
        sq = mom[p] * mom[p]
        lanes = sq[:, :128]
        for k in range(1, sq.shape[1] // 128):
            lanes = lanes + sq[:, k * 128 : (k + 1) * 128]
        acc = lanes[:8]
        for k in range(1, share // 8):
            acc = acc + lanes[k * 8 : (k + 1) * 8]
        nrm[p, me] = acc
        for k in range(7):
            to_norms(p, k).start()

    def sum_norms(p):
        settle(nrm.at[p, :7], n_r.at[p])
        acc = nrm[p, 0]
        for k in range(1, 8):
            acc = acc + nrm[p, k]
        total_sq[p] = acc

    def finish(p):
        sum_norms(p)
        settle(full.at[p, :3], d_r.at[p])

    open_line(0)
    open_line(1)
    open_line(2, 0)
    open_line(3, 0)
    for p in range(2):
        loads[2 + p].wait()
        swap_cot(p).start()
    loads[6].wait()
    loads[7].wait()
    old[1] = mo[...].T
    for p in range(2):
        loads[4 + p].wait()
        own[p] = slab_dot(p, f, slice(None))
        settle(cot.at[p, ot], cx_r.at[p])
    run_line(0, 0)
    run_line(1, 0)
    open_line(2, 1)
    run_line(0, 1)
    run_line(1, 1)
    open_line(2, 2)
    run_line(0, 2)
    run_line(1, 2)
    run_line(2, 0)
    open_line(3, 1)
    run_line(2, 1)
    open_line(3, 2)
    project(0, (0, 1))
    run_line(2, 2)
    scatter_reps(0)
    scatter_reps(1)
    run_line(3, 0)
    project(1, (2,))
    run_line(3, 1)
    run_line(3, 2)
    scatter_reps(2)
    scatter_tokens(0)
    scatter_tokens(1)
    project(1, (3,))
    scatter_reps(3)
    gather_sums(0)
    scatter_tokens(2)
    gather_sums(1)
    scatter_tokens(3)
    gather_dirs(0)
    gather_sums(2)
    gather_dirs(1)
    send_norms(0)
    gather_sums(3)
    gather_dirs(2)
    gather_dirs(3)
    send_norms(1)
    finish(0)
    finish(1)
    inner = (f > 0) & (f < last)

    @pl.when(inner)
    def _():
        settle(gath.at[0, :2], sent.at[0])
        settle(gath.at[0, :3], sent.at[1])

    @pl.when(jnp.logical_not(inner))
    def _():
        settle(gath.at[0, :1], sent.at[0])

    settle(gath.at[0, :3], sent.at[2])
    settle(cot.at[0], sent.at[3])

    @pl.when(t != y)
    def _():
        settle(pb, sent.at[4])

    @pl.when(t == y)
    def _():
        settle(pb.at[:3], sent.at[4])

    settle(t2, sent.at[5])
    settle(t2, sent.at[6])
    settle(full.at[:, :3], sent.at[7])
    settle(nrm.at[:, :7], sent.at[8])


def finish_kernel(
    entries, qb, ob, fq, fo, sq, qw, ow, mq, mo,
    qs_o, os_o, qn_o, on_o, qc_o, oc_o, mq_o, mo_o,
):
    def scale(p):
        rows = jnp.sum(sq[p], axis=0, keepdims=True)
        return lax.rsqrt(jnp.sum(rows, axis=1, keepdims=True) / entries + EPS)

    step = jnp.dot(qb[...], fq[0], preferred_element_type=jnp.float32) * scale(0)
    new = qw[...] - RATE * step
    qs_o[...] = step
    qn_o[...] = new
    qc_o[...] = new.astype(jnp.bfloat16)
    step = lax.dot_general(
        fo[0].T, ob[...], (((1,), (1,)), ((), ())), preferred_element_type=jnp.float32
    ) * scale(1)
    new = ow[...] - RATE * step
    os_o[...] = step
    on_o[...] = new
    oc_o[...] = new.astype(jnp.bfloat16)
    mq_o[...] = mq[0]
    mo_o[...] = mo[0].T


def on_device_fast(
    saved_input, query_cot, attn_out, out_cot, query_basis, output_basis,
    query_weight, output_weight, query_moment, output_moment,
):
    tokens, depth_all = saved_input.shape
    width = query_cot.shape[1]
    depth, rank = query_basis.shape
    share = rank // 4
    cut = share // 2
    piece = cut // 4
    entries = rank * width * lax.axis_size("tp")
    bf, f32 = jnp.bfloat16, jnp.float32
    any_spec = pl.BlockSpec(memory_space=pl.ANY)
    dma = pltpu.SemaphoreType.DMA
    ins = (
        saved_input, out_cot, query_cot, attn_out, query_basis, output_basis,
        query_moment, output_moment,
    )
    full, mom, norm = pl.pallas_call(
        exchange_kernel,
        out_shape=(
            jax.ShapeDtypeStruct((2, 4, share, width), bf),
            jax.ShapeDtypeStruct((2, share, width), f32),
            jax.ShapeDtypeStruct((2, 8, 128), f32),
        ),
        in_specs=[any_spec] * 8,
        out_specs=(pl.BlockSpec(memory_space=pltpu.VMEM),) * 3,
        scratch_shapes=[
            pltpu.VMEM((2, tokens, depth_all), bf),
            pltpu.VMEM((2, 2, tokens, width), bf),
            pltpu.VMEM((2, depth, rank // 2), bf),
            pltpu.VMEM((2, share, width), f32),
            pltpu.VMEM((width, share), f32),
            pltpu.VMEM((2, 4, depth, 2 * share), bf),
            pltpu.VMEM((2, tokens, 2 * share), f32),
            pltpu.VMEM((UNITS, 2, 2, cut, width), bf),
            pltpu.VMEM((UNITS, 4, cut, width), bf),
            pltpu.VMEM((UNITS, 4, piece, width), bf),
            pltpu.VMEM((UNITS, 3, piece, width), bf),
            pltpu.VMEM((UNITS, 4, piece, width), bf),
            pltpu.VMEM((2, 8, 8, 128), f32),
            dma((8,)), dma((9,)), dma((2,)), dma((UNITS, 3)), dma((UNITS,)), dma((UNITS,)),
            dma((UNITS,)), dma((UNITS, 3)), dma((2,)), dma((2,)),
        ],
        compiler_params=pltpu.CompilerParams(
            collective_id=0, has_side_effects=True, vmem_limit_bytes=20 * 2**20
        ),
    )(*(pltpu.with_memory_space_constraint(a, pltpu.HBM) for a in ins))
    full = full.reshape(2, rank, width)
    n = 4
    rows = pl.BlockSpec((depth // n, rank), lambda i: (i, 0))
    whole = pl.BlockSpec((depth, rank), lambda i: (0, 0))
    wq = pl.BlockSpec((depth // n, width), lambda i: (i, 0))
    wo = pl.BlockSpec((width // n, depth), lambda i: (i, 0))
    mq = pl.BlockSpec((share // n, width), lambda i: (i, 0))
    mo = pl.BlockSpec((width // n, share), lambda i: (i, 0))
    sq, so = query_weight.shape, output_weight.shape
    return pl.pallas_call(
        functools.partial(finish_kernel, entries),
        grid=(n,),
        out_shape=tuple(
            jax.ShapeDtypeStruct(s, d)
            for s, d in (
                (sq, f32), (so, f32), (sq, f32), (so, f32), (sq, bf), (so, bf),
                (query_moment.shape, f32), (output_moment.shape, f32),
            )
        ),
        in_specs=[
            rows, whole,
            pl.BlockSpec((1, rank, width), lambda i: (0, 0, 0)),
            pl.BlockSpec((1, rank, width // n), lambda i: (1, 0, i)),
            pl.BlockSpec((2, 8, 128), lambda i: (0, 0, 0)),
            wq, wo,
            pl.BlockSpec((1, share // n, width), lambda i: (0, i, 0)),
            pl.BlockSpec((1, share, width // n), lambda i: (1, 0, i)),
        ],
        out_specs=(wq, wo, wq, wo, wq, wo, mq, mo),
        cost_estimate=pl.CostEstimate(
            flops=4 * depth * rank * width, bytes_accessed=20 * depth * width, transcendentals=0
        ),
        compiler_params=pltpu.CompilerParams(vmem_limit_bytes=20 * 2**20),
    )(query_basis, output_basis, full, full, norm, query_weight, output_weight, mom, mom)


def solution(mesh):
    small = dict(mesh.shape) == {"fs": 4, "rep": 4, "tp": 2}
    body = on_device_fast if small else on_device
    placed = (
        P(("fs", "rep"), None),
        P(("fs", "rep"), "tp"),
        P(("fs", "rep"), "tp"),
        P(("fs", "rep"), None),
        P("fs", None),
        P("fs", None),
        P("fs", "tp"),
        P("tp", "fs"),
        P("rep", "tp"),
        P("tp", "rep"),
    )
    return jax.shard_map(
        body,
        mesh=mesh,
        in_specs=placed,
        out_specs=(
            P("fs", "tp"),
            P("tp", "fs"),
            P("fs", "tp"),
            P("tp", "fs"),
            P("fs", "tp"),
            P("tp", "fs"),
            P("rep", "tp"),
            P("tp", "rep"),
        ),
        check_vma=False,
    )
```

```python
import functools

import jax
import jax.numpy as jnp
from jax import lax
from jax.experimental import pallas as pl
from jax.experimental.pallas import tpu as pltpu
from jax.sharding import PartitionSpec as P

BETA = 0.8
RATE = 0.2
EPS = 1e-06


def on_device(
    saved_input,
    query_cot,
    attn_out,
    out_cot,
    query_basis,
    output_basis,
    query_weight,
    output_weight,
    query_moment,
    output_moment,
):
    rank = query_basis.shape[1]
    grad_rows = lax.psum_scatter(
        jnp.dot(saved_input.T, query_cot, preferred_element_type=jnp.float32),
        "fs",
        scatter_dimension=0,
        tiled=True,
    )
    query_part = jnp.dot(
        query_basis.astype(jnp.float32).T, grad_rows, precision=lax.Precision.HIGHEST
    )
    cot_proj = jnp.dot(
        out_cot,
        lax.all_gather(output_basis, "fs", axis=0, tiled=True),
        preferred_element_type=jnp.float32,
    )
    output_part = jnp.dot(attn_out.astype(jnp.float32).T, cot_proj, precision=lax.Precision.HIGHEST)
    reps = lax.axis_size("rep")
    share = rank // reps
    query_terms, output_terms = (
        lax.all_to_all(
            query_part.astype(jnp.bfloat16), "rep", split_axis=0, concat_axis=0, tiled=True
        ).astype(query_part.dtype),
        lax.all_to_all(
            output_part.T.astype(jnp.bfloat16), "rep", split_axis=0, concat_axis=0, tiled=True
        ).astype(jnp.float32),
    )
    width = query_part.shape[1]
    query_local = jnp.sum(query_terms.reshape(reps, share, width), axis=0)
    output_local = jnp.sum(output_terms.reshape(reps, share, width), axis=0)
    query_share, output_flip = lax.psum((query_local, output_local), "fs")
    output_share = output_flip.T
    query_moment_new = BETA * query_moment + (1.0 - BETA) * query_share
    output_moment_new = BETA * output_moment + (1.0 - BETA) * output_share
    query_squares, output_squares = lax.psum(
        (
            jnp.sum(query_moment_new * query_moment_new),
            jnp.sum(output_moment_new * output_moment_new),
        ),
        ("rep", "tp"),
    )
    entries = rank * query_moment.shape[1] * lax.axis_size("tp")
    query_dir = (query_moment_new * lax.rsqrt(query_squares / entries + EPS)).astype(jnp.bfloat16)
    output_dir = (output_moment_new * lax.rsqrt(output_squares / entries + EPS)).astype(
        jnp.bfloat16
    )
    query_full, output_full = (
        lax.all_gather(query_dir, "rep", axis=0, tiled=True),
        lax.all_gather(output_dir, "rep", axis=1, tiled=True),
    )
    query_step = jnp.dot(query_basis, query_full, preferred_element_type=jnp.float32)
    output_step = jnp.dot(output_full, output_basis.T, preferred_element_type=jnp.float32)
    query_new = query_weight - RATE * query_step
    output_new = output_weight - RATE * output_step
    return (
        query_step,
        output_step,
        query_new,
        output_new,
        query_new.astype(jnp.bfloat16),
        output_new.astype(jnp.bfloat16),
        query_moment_new,
        output_moment_new,
    )


MESH = pl.DeviceIdType.MESH
UNITS = 4


def exchange_kernel(
    si_hbm, oc_hbm, qc_hbm, ao_hbm, qb_hbm, ob_hbm, mq_hbm, mo_hbm,
    full, mom, total_sq,
    act, cot, head, base, old, mo, gath, own, pb, t1, sb, t2, ag, nrm, zb, zt, yb, yt,
    load_sem, sent, cx_r, az_r, aw_r, b1_r, b2_r, g_r, n_r, d_r, z_r,
):
    f, r, t = lax.axis_index("fs"), lax.axis_index("rep"), lax.axis_index("tp")
    y, x = r // 2, r % 2
    ot = 1 - t
    fpeer = [(f + d) % 4 for d in (1, 3, 2)]
    fsrc = [(f + 4 - d) % 4 for d in (1, 3, 2)]
    rpeer = [2 * y + (1 - x), 2 * (1 - y) + x, 3 - r]
    depth, half = base.shape[1], base.shape[2]
    hd = depth // 2
    qd = depth // 4
    share = half // 2
    cut = share // 2
    piece = cut // 4

    cols = pl.ds(pl.multiple_of(t * half, half), half)
    first = pl.ds(pl.multiple_of(r * qd, qd), qd)
    loads = []
    for k, (src, dst) in enumerate((
        (qb_hbm.at[first, cols], head), (qb_hbm.at[:, cols], base.at[0]), (ob_hbm.at[:, cols], base.at[1]),
        (qc_hbm, cot.at[0, t]), (ao_hbm, cot.at[1, t]),
        (si_hbm, act.at[0]), (oc_hbm, act.at[1]),
        (mq_hbm, old.at[0]), (mo_hbm, mo),
    )):
        c = pltpu.make_async_copy(src, dst, load_sem.at[k])
        c.start()
        loads.append(c)

    barrier = pltpu.get_barrier_semaphore()
    for g in fpeer:
        pl.semaphore_signal(barrier, inc=1, device_id=(g, r, t), device_id_type=MESH)
    for q in rpeer:
        for s in (t, ot):
            pl.semaphore_signal(barrier, inc=1, device_id=(f, q, s), device_id_type=MESH)
    pl.semaphore_signal(barrier, inc=1, device_id=(f, r, ot), device_id_type=MESH)

    def deal(p, rows, block):
        lo, hi = block[:, :share], block[:, share:]
        gath[p, f, rows, :share] = jnp.concatenate([lo[:, :cut], hi[:, :cut]], axis=1)
        gath[p, f, rows, share:] = jnp.concatenate([lo[:, cut:], hi[:, cut:]], axis=1)

    loads[0].wait()
    deal(0, first, head[...])
    pl.semaphore_wait(barrier, 10)

    def remote(src, dst, ss, rs, dev):
        return pltpu.make_async_remote_copy(
            src_ref=src, dst_ref=dst, send_sem=ss, recv_sem=rs, device_id=dev, device_id_type=MESH
        )

    def settle(ref, sem):
        pltpu.make_async_copy(ref, ref, sem).wait()

    h = x * (1 - t) + y * t
    near = rpeer[0] * (1 - t) + rpeer[1] * t
    mine = (
        first,
        pl.ds(pl.multiple_of(h * hd, hd), hd),
    )
    last = 3

    def unit_ref(u, slab):
        k = u % 2
        return gath.at[u // 2, slab, mine[u // 2], k * share : (k + 1) * share]

    def line(u, way, s, arrive=False):
        step = -1 if way == 0 else 1
        slab = f + step * s + (step if arrive else 0)
        ref = unit_ref(u, slab)
        dev = f + step if arrive else f - step
        to = f if arrive else dev
        slot = s if way == 0 else to + s
        return remote(ref, ref, sent.at[min(s, 1)], az_r.at[u, slot], (dev, r, t))

    def sends_line(way, s):
        return (f >= s) & (f < last) if way == 0 else (f + s <= last) & (f > 0)

    def gets_line(way, s):
        return f >= s + 1 if way == 0 else f + s + 1 <= last

    def carried(way):
        return f if way == 0 else last - f

    def share_slab(u, slab):
        ref = unit_ref(u, slab)
        for q in (rpeer[2], rpeer[0], rpeer[1]) if u < 2 else (near,):
            remote(ref, ref, sent.at[2 if u < 2 else 9], aw_r.at[u], (f, q, t)).start()

    def open_line(u, last_only=None):
        for way in range(2):
            go = sends_line(way, 0)
            if last_only is not None:
                go = go & ((carried(way) == 0) == last_only)

            @pl.when(go)
            def _():
                line(u, way, 0).start()

    def run_line(u, s):
        for way in range(2):
            @pl.when(gets_line(way, s))
            def _():
                line(u, way, s, True).wait_recv()
            if s < 2:
                @pl.when(sends_line(way, s + 1))
                def _():
                    line(u, way, s + 1).start()

            @pl.when(gets_line(way, s))
            def _():
                slab = f - 1 - s if way == 0 else f + 1 + s
                share_slab(u, slab)

    def swap_cot(p):
        ref = cot.at[p, t]
        return remote(ref, ref, sent.at[3], cx_r.at[p], (f, r, ot))

    def to_reps(u, k):
        j = 1 - x if k < 2 else x
        c = (0, 1, ot, t)[k]
        return remote(
            pb.at[u - 1, j, c], t1.at[u, r], sent.at[4], b1_r.at[u], (f, 2 * t + j, c)
        )

    def scatter_zs():
        for k in (2, 0, 1):
            remote(
                zb.at[fpeer[k]], zt.at[k], sent.at[10], z_r.at[0], (fpeer[k], r, t)
            ).start()

    def to_owner(k):
        j = 1 - x if k < 2 else x
        c = (0, 1, ot, t)[k]
        return remote(yb.at[j, c], yt.at[r], sent.at[11], z_r.at[1], (f, 2 * t + j, c))

    def scatter_owners():
        settle(zt, z_r.at[0])
        total = zb[f].astype(jnp.float32)
        for k in range(3):
            total = total + zt[k].astype(jnp.float32)
        yb[...] = total.astype(jnp.bfloat16)
        for k in range(3):
            to_owner(k).start()

        @pl.when(t != y)
        def _():
            to_owner(3).start()

        @pl.when(t == y)
        def _():
            yt[r] = yb[x, t]

    def spread_own():
        @pl.when(t != y)
        def _():
            settle(yt, z_r.at[1])

        @pl.when(t == y)
        def _():
            settle(yt.at[:3], z_r.at[1])

        total = yt[0].astype(jnp.float32)
        for q in range(1, 4):
            total = total + yt[q].astype(jnp.float32)
        send_sums(0, total)

    def spread_sums():
        for k in range(3):
            settle(ag.at[2, fsrc[k]], g_r.at[2, k])
            update_own(2, fsrc[k])

    def spread_zs():
        rows = rows_at(2, f)
        settle(full.at[1, :3, rows, :], z_r.at[2])
        for k in (2, 0, 1):
            for q in rpeer:
                ref = full.at[1, q, rows, :]
                remote(ref, ref, sent.at[12], z_r.at[3], (fpeer[k], r, t)).start()

    def slab_dot(p, g, lanes):
        at = pl.ds(pl.multiple_of(g * depth, depth), depth)
        return jnp.dot(act[p, :, at], gath[p, g, :, lanes], preferred_element_type=jnp.float32)

    def project(p, us):
        for u in us:
            k = u % 2
            settle(
                gath.at[p, :3, : depth - (qd, hd)[p], k * share : (k + 1) * share], aw_r.at[u]
            )
        lanes = slice((us[0] % 2) * share, (us[-1] % 2 + 1) * share)
        part = own[p, :, lanes]
        for g in fsrc:
            part = part + slab_dot(p, g, lanes)
        part = part.astype(jnp.bfloat16)
        for i, u in reversed(tuple(enumerate(us))):
            for c in range(2):
                terms = lax.dot_general(
                    part[:, i * share : (i + 1) * share], cot[p, c], (((0,), (0,)), ((), ())),
                    preferred_element_type=jnp.float32,
                )
                for j in range(2):
                    block = terms[j * cut : (j + 1) * cut].astype(jnp.bfloat16)
                    if u > 0:
                        pb[u - 1, j, c] = block
                    else:
                        for g in range(4):
                            zb[g, j, c] = block[g * piece : (g + 1) * piece]
            if u > 0:
                scatter_reps(u)
            else:
                scatter_zs()

    def scatter_reps(u):
        for k in range(3):
            to_reps(u, k).start()

        @pl.when(t != y)
        def _():
            to_reps(u, 3).start()

        @pl.when(t == y)
        def _():
            t1[u, r] = pb[u - 1, x, t]

    def scatter_tokens(u):
        @pl.when(t != y)
        def _():
            settle(t1.at[u], b1_r.at[u])

        @pl.when(t == y)
        def _():
            settle(t1.at[u, :3], b1_r.at[u])

        total = t1[u, 0].astype(jnp.float32)
        for q in range(1, 4):
            total = total + t1[u, q].astype(jnp.float32)
        for g in range(4):
            sb[u, g] = total[g * piece : (g + 1) * piece].astype(jnp.bfloat16)
        for k in (2, 0, 1):
            to_token(u, k).start()

    def to_token(u, k):
        return remote(
            sb.at[u, fpeer[k]], t2.at[u, k], sent.at[5], b2_r.at[u], (fpeer[k], r, t)
        )

    def rows_at(u, g):
        at = (u % 2) * cut + g * piece
        return pl.ds(pl.multiple_of(at, piece), piece)

    def to_dirs(u, g, k):
        ref = full.at[u // 2, r, rows_at(u, g), :]
        ss, rs = (sent.at[12], z_r.at[2]) if u == 2 else (sent.at[7], d_r.at[u // 2])
        return remote(ref, ref, ss, rs, (f, rpeer[k], t))

    def to_sums(u, k):
        return remote(
            ag.at[u, f], ag.at[u, f], sent.at[6], g_r.at[u, k], (fpeer[k], r, t)
        )

    def update_own(u, g):
        p, rows = u // 2, rows_at(u, g)
        new = BETA * old[p, rows, :] + (1.0 - BETA) * ag[u, g].astype(jnp.float32)
        mom[p, rows, :] = new
        full[p, r, rows, :] = new.astype(jnp.bfloat16)

    def update(u, g):
        update_own(u, g)
        for k in (2, 0, 1):
            to_dirs(u, g, k).start()

    def send_sums(u, total):
        ag[u, f] = total.astype(jnp.bfloat16)
        for k in (2, 0, 1):
            to_sums(u, k).start()
        update(u, f)

    def gather_sums(u):
        total = sb[u, f].astype(jnp.float32)
        settle(t2.at[u], b2_r.at[u])
        for k in range(3):
            total = total + t2[u, k].astype(jnp.float32)
        send_sums(u, total)

    def gather_dirs(u):
        for k in range(3):
            settle(ag.at[u, fsrc[k]], g_r.at[u, k])
            update(u, fsrc[k])

    others = [(q, s) for q in rpeer for s in (t, ot)] + [(r, ot)]
    me = 2 * r + t

    def to_norms(p, k):
        q, s = others[k]
        ref = nrm.at[p, me]
        return remote(ref, ref, sent.at[8], n_r.at[p], (f, q, s))

    def send_norms(p):
        sq = mom[p] * mom[p]
        lanes = sq[:, :128]
        for k in range(1, sq.shape[1] // 128):
            lanes = lanes + sq[:, k * 128 : (k + 1) * 128]
        acc = lanes[:8]
        for k in range(1, share // 8):
            acc = acc + lanes[k * 8 : (k + 1) * 8]
        nrm[p, me] = acc
        for k in range(7):
            to_norms(p, k).start()

    def sum_norms(p):
        settle(nrm.at[p, :7], n_r.at[p])
        acc = nrm[p, 0]
        for k in range(1, 8):
            acc = acc + nrm[p, k]
        total_sq[p] = acc

    def finish(p):
        sum_norms(p)
        if p == 0:
            settle(full.at[0, :3], d_r.at[0])
        else:
            settle(full.at[1, :3, : 3 * piece, :], z_r.at[3])
            settle(full.at[1, :3, :cut, :], d_r.at[1])

    open_line(0)
    open_line(1)
    loads[2].wait()
    deal(1, slice(None), base[1])
    open_line(2)
    open_line(3, True)
    loads[1].wait()
    for k in range(1, 4):
        rows = pl.ds(pl.multiple_of((r + k) % 4 * qd, qd), qd)
        deal(0, rows, base[0, rows, :])
    for p in range(2):
        loads[3 + p].wait()
        swap_cot(p).start()
    loads[7].wait()
    loads[8].wait()
    old[1] = mo[...].T
    for p in range(2):
        loads[5 + p].wait()
        own[p] = slab_dot(p, f, slice(None))
        settle(cot.at[p, ot], cx_r.at[p])
    run_line(0, 0)
    run_line(1, 0)
    open_line(3, False)
    run_line(0, 1)
    run_line(1, 1)
    run_line(2, 0)
    run_line(0, 2)
    run_line(1, 2)
    run_line(3, 0)
    run_line(2, 1)
    run_line(2, 2)
    run_line(3, 1)
    run_line(3, 2)
    project(0, (0, 1))
    project(1, (2,))
    project(1, (3,))
    scatter_tokens(1)
    scatter_tokens(2)
    scatter_owners()
    gather_sums(1)
    scatter_tokens(3)
    gather_sums(2)
    spread_own()
    gather_dirs(1)
    gather_sums(3)
    spread_zs()
    spread_sums()
    gather_dirs(0)
    send_norms(0)
    gather_dirs(3)
    send_norms(1)
    finish(0)
    finish(1)
    inner = (f > 0) & (f < last)

    @pl.when(inner)
    def _():
        settle(gath.at[0, :3, :, :share], sent.at[0])
        settle(gath.at[0, :3, : depth - qd], sent.at[1])

    @pl.when(jnp.logical_not(inner))
    def _():
        settle(gath.at[0, :3, :hd, :share], sent.at[0])

    for k in range(2):
        settle(gath.at[k, :3, : depth - (qd, hd)[k], :], sent.at[2 + 7 * k])
    settle(cot.at[0], sent.at[3])

    @pl.when(t != y)
    def _():
        settle(pb, sent.at[4])
        settle(yt, sent.at[11])

    @pl.when(t == y)
    def _():
        settle(pb.at[:, :, :, : 3 * piece], sent.at[4])
        settle(yt.at[:3], sent.at[11])

    settle(t2.at[:3], sent.at[5])
    settle(t2, sent.at[6])
    settle(full.at[:, :3, : 6 * piece], sent.at[7])
    settle(nrm.at[:, :7], sent.at[8])
    settle(zt, sent.at[10])
    settle(t2, sent.at[12])


def finish_kernel(
    entries, qb, ob, fq, fo, sq, qw, ow, mq, mo,
    qs_o, os_o, qn_o, on_o, qc_o, oc_o, mq_o, mo_o,
):
    def scale(p):
        rows = jnp.sum(sq[p], axis=0, keepdims=True)
        return lax.rsqrt(jnp.sum(rows, axis=1, keepdims=True) / entries + EPS)

    step = jnp.dot(qb[...], fq[0], preferred_element_type=jnp.float32) * scale(0)
    new = qw[...] - RATE * step
    qs_o[...] = step
    qn_o[...] = new
    qc_o[...] = new.astype(jnp.bfloat16)
    step = lax.dot_general(
        fo[0].T, ob[...], (((1,), (1,)), ((), ())), preferred_element_type=jnp.float32
    ) * scale(1)
    new = ow[...] - RATE * step
    os_o[...] = step
    on_o[...] = new
    oc_o[...] = new.astype(jnp.bfloat16)
    mq_o[...] = mq[0]
    mo_o[...] = mo[0].T


def on_device_fast(
    saved_input, query_cot, attn_out, out_cot, query_basis, output_basis,
    query_weight, output_weight, query_moment, output_moment,
):
    tokens, depth_all = saved_input.shape
    width = query_cot.shape[1]
    depth, rank = query_basis.shape
    share = rank // 4
    cut = share // 2
    piece = cut // 4
    entries = rank * width * lax.axis_size("tp")
    bf, f32 = jnp.bfloat16, jnp.float32
    any_spec = pl.BlockSpec(memory_space=pl.ANY)
    dma = pltpu.SemaphoreType.DMA
    ins = (
        saved_input, out_cot, query_cot, attn_out, query_basis, output_basis,
        query_moment, output_moment,
    )
    full, mom, norm = pl.pallas_call(
        exchange_kernel,
        out_shape=(
            jax.ShapeDtypeStruct((2, 4, share, width), bf),
            jax.ShapeDtypeStruct((2, share, width), f32),
            jax.ShapeDtypeStruct((2, 8, 128), f32),
        ),
        in_specs=[any_spec] * 8,
        out_specs=(pl.BlockSpec(memory_space=pltpu.VMEM),) * 3,
        scratch_shapes=[
            pltpu.VMEM((2, tokens, depth_all), bf),
            pltpu.VMEM((2, 2, tokens, width), bf),
            pltpu.VMEM((depth // 4, rank // 2), bf),
            pltpu.VMEM((2, depth, rank // 2), bf),
            pltpu.VMEM((2, share, width), f32),
            pltpu.VMEM((width, share), f32),
            pltpu.VMEM((2, 4, depth, 2 * share), bf),
            pltpu.VMEM((2, tokens, 2 * share), f32),
            pltpu.VMEM((UNITS - 1, 2, 2, cut, width), bf),
            pltpu.VMEM((UNITS, 4, cut, width), bf),
            pltpu.VMEM((UNITS, 4, piece, width), bf),
            pltpu.VMEM((UNITS, 3, piece, width), bf),
            pltpu.VMEM((UNITS, 4, piece, width), bf),
            pltpu.VMEM((2, 8, 8, 128), f32),
            pltpu.VMEM((4, 2, 2, piece, width), bf),
            pltpu.VMEM((3, 2, 2, piece, width), bf),
            pltpu.VMEM((2, 2, piece, width), bf),
            pltpu.VMEM((4, piece, width), bf),
            dma((9,)), dma((13,)), dma((2,)), dma((UNITS, 3)), dma((UNITS,)), dma((UNITS,)),
            dma((UNITS,)), dma((UNITS, 3)), dma((2,)), dma((2,)), dma((4,)),
        ],
        compiler_params=pltpu.CompilerParams(
            collective_id=0, has_side_effects=True, vmem_limit_bytes=20 * 2**20
        ),
    )(*(pltpu.with_memory_space_constraint(a, pltpu.HBM) for a in ins))
    full = full.reshape(2, rank, width)
    n = 2
    rows = pl.BlockSpec((depth // n, rank), lambda i: (i, 0))
    whole = pl.BlockSpec((depth, rank), lambda i: (0, 0))
    wq = pl.BlockSpec((depth // n, width), lambda i: (i, 0))
    wo = pl.BlockSpec((width // n, depth), lambda i: (i, 0))
    mq = pl.BlockSpec((share // n, width), lambda i: (i, 0))
    mo = pl.BlockSpec((width // n, share), lambda i: (i, 0))
    sq, so = query_weight.shape, output_weight.shape
    return pl.pallas_call(
        functools.partial(finish_kernel, entries),
        grid=(n,),
        out_shape=tuple(
            jax.ShapeDtypeStruct(s, d)
            for s, d in (
                (sq, f32), (so, f32), (sq, f32), (so, f32), (sq, bf), (so, bf),
                (query_moment.shape, f32), (output_moment.shape, f32),
            )
        ),
        in_specs=[
            rows, whole,
            pl.BlockSpec((1, rank, width), lambda i: (0, 0, 0)),
            pl.BlockSpec((1, rank, width // n), lambda i: (1, 0, i)),
            pl.BlockSpec((2, 8, 128), lambda i: (0, 0, 0)),
            wq, wo,
            pl.BlockSpec((1, share // n, width), lambda i: (0, i, 0)),
            pl.BlockSpec((1, share, width // n), lambda i: (1, 0, i)),
        ],
        out_specs=(wq, wo, wq, wo, wq, wo, mq, mo),
        cost_estimate=pl.CostEstimate(
            flops=4 * depth * rank * width, bytes_accessed=20 * depth * width, transcendentals=0
        ),
        compiler_params=pltpu.CompilerParams(vmem_limit_bytes=20 * 2**20),
    )(query_basis, output_basis, full, full, norm, query_weight, output_weight, mom, mom)


def solution(mesh):
    small = dict(mesh.shape) == {"fs": 4, "rep": 4, "tp": 2}
    body = on_device_fast if small else on_device
    placed = (
        P(("fs", "rep"), None),
        P(("fs", "rep"), "tp"),
        P(("fs", "rep"), "tp"),
        P(("fs", "rep"), None),
        P("fs", None),
        P("fs", None),
        P("fs", "tp"),
        P("tp", "fs"),
        P("rep", "tp"),
        P("tp", "rep"),
    )
    return jax.shard_map(
        body,
        mesh=mesh,
        in_specs=placed,
        out_specs=(
            P("fs", "tp"),
            P("tp", "fs"),
            P("fs", "tp"),
            P("tp", "fs"),
            P("fs", "tp"),
            P("tp", "fs"),
            P("rep", "tp"),
            P("tp", "rep"),
        ),
        check_vma=False,
    )
```

```python
import functools

import jax
import jax.numpy as jnp
from jax import lax
from jax.experimental import pallas as pl
from jax.experimental.pallas import tpu as pltpu
from jax.sharding import PartitionSpec as P

BETA = 0.8
RATE = 0.2
EPS = 1e-06


def on_device(
    saved_input,
    query_cot,
    attn_out,
    out_cot,
    query_basis,
    output_basis,
    query_weight,
    output_weight,
    query_moment,
    output_moment,
):
    rank = query_basis.shape[1]
    grad_rows = lax.psum_scatter(
        jnp.dot(saved_input.T, query_cot, preferred_element_type=jnp.float32),
        "fs",
        scatter_dimension=0,
        tiled=True,
    )
    query_part = jnp.dot(
        query_basis.astype(jnp.float32).T, grad_rows, precision=lax.Precision.HIGHEST
    )
    cot_proj = jnp.dot(
        out_cot,
        lax.all_gather(output_basis, "fs", axis=0, tiled=True),
        preferred_element_type=jnp.float32,
    )
    output_part = jnp.dot(attn_out.astype(jnp.float32).T, cot_proj, precision=lax.Precision.HIGHEST)
    reps = lax.axis_size("rep")
    share = rank // reps
    query_terms, output_terms = (
        lax.all_to_all(
            query_part.astype(jnp.bfloat16), "rep", split_axis=0, concat_axis=0, tiled=True
        ).astype(query_part.dtype),
        lax.all_to_all(
            output_part.T.astype(jnp.bfloat16), "rep", split_axis=0, concat_axis=0, tiled=True
        ).astype(jnp.float32),
    )
    width = query_part.shape[1]
    query_local = jnp.sum(query_terms.reshape(reps, share, width), axis=0)
    output_local = jnp.sum(output_terms.reshape(reps, share, width), axis=0)
    query_share, output_flip = lax.psum((query_local, output_local), "fs")
    output_share = output_flip.T
    query_moment_new = BETA * query_moment + (1.0 - BETA) * query_share
    output_moment_new = BETA * output_moment + (1.0 - BETA) * output_share
    query_squares, output_squares = lax.psum(
        (
            jnp.sum(query_moment_new * query_moment_new),
            jnp.sum(output_moment_new * output_moment_new),
        ),
        ("rep", "tp"),
    )
    entries = rank * query_moment.shape[1] * lax.axis_size("tp")
    query_dir = (query_moment_new * lax.rsqrt(query_squares / entries + EPS)).astype(jnp.bfloat16)
    output_dir = (output_moment_new * lax.rsqrt(output_squares / entries + EPS)).astype(
        jnp.bfloat16
    )
    query_full, output_full = (
        lax.all_gather(query_dir, "rep", axis=0, tiled=True),
        lax.all_gather(output_dir, "rep", axis=1, tiled=True),
    )
    query_step = jnp.dot(query_basis, query_full, preferred_element_type=jnp.float32)
    output_step = jnp.dot(output_full, output_basis.T, preferred_element_type=jnp.float32)
    query_new = query_weight - RATE * query_step
    output_new = output_weight - RATE * output_step
    return (
        query_step,
        output_step,
        query_new,
        output_new,
        query_new.astype(jnp.bfloat16),
        output_new.astype(jnp.bfloat16),
        query_moment_new,
        output_moment_new,
    )


MESH = pl.DeviceIdType.MESH
UNITS = 4


def exchange_kernel(
    si_hbm, oc_hbm, qc_hbm, ao_hbm, qb_hbm, ob_hbm, mq_hbm, mo_hbm,
    full, mom, total_sq,
    act, cot, head, base, old, mo, gath, own, pb, t1, sb, t2, ag, nrm, zb, zt, yb, yt,
    load_sem, sent, cx_r, az_r, aw_r, b1_r, b2_r, g_r, n_r, d_r, z_r,
):
    f, r, t = lax.axis_index("fs"), lax.axis_index("rep"), lax.axis_index("tp")
    y, x = r // 2, r % 2
    ot = 1 - t
    fpeer = [3 - f, (f + 2) % 4, f + 1 - 2 * (f % 2)]
    rpeer = [2 * y + (1 - x), 2 * (1 - y) + x, 3 - r]
    depth, half = base.shape[1], base.shape[2]
    hd = depth // 2
    qd = depth // 4
    share = half // 2
    cut = share // 2
    piece = cut // 4

    cols = pl.ds(pl.multiple_of(t * half, half), half)
    first = pl.ds(pl.multiple_of(r * qd, qd), qd)
    loads = []
    for k, (src, dst) in enumerate((
        (qb_hbm.at[first, cols], head), (qb_hbm.at[:, cols], base.at[0]), (ob_hbm.at[:, cols], base.at[1]),
        (qc_hbm, cot.at[0, t]), (ao_hbm, cot.at[1, t]),
        (si_hbm, act.at[0]), (oc_hbm, act.at[1]),
        (mq_hbm, old.at[0]), (mo_hbm, mo),
    )):
        c = pltpu.make_async_copy(src, dst, load_sem.at[k])
        c.start()
        loads.append(c)

    barrier = pltpu.get_barrier_semaphore()
    for g in fpeer:
        pl.semaphore_signal(barrier, inc=1, device_id=(g, r, t), device_id_type=MESH)
    for q in rpeer:
        for s in (t, ot):
            pl.semaphore_signal(barrier, inc=1, device_id=(f, q, s), device_id_type=MESH)
    pl.semaphore_signal(barrier, inc=1, device_id=(f, r, ot), device_id_type=MESH)

    def deal(p, rows, block):
        lo, hi = block[:, :share], block[:, share:]
        gath[p, f, rows, :share] = jnp.concatenate([lo[:, :cut], hi[:, :cut]], axis=1)
        gath[p, f, rows, share:] = jnp.concatenate([lo[:, cut:], hi[:, cut:]], axis=1)

    loads[0].wait()
    deal(0, first, head[...])
    pl.semaphore_wait(barrier, 10)

    def remote(src, dst, ss, rs, dev):
        return pltpu.make_async_remote_copy(
            src_ref=src, dst_ref=dst, send_sem=ss, recv_sem=rs, device_id=dev, device_id_type=MESH
        )

    def settle(ref, sem):
        pltpu.make_async_copy(ref, ref, sem).wait()

    h = x * (1 - t) + y * t
    near = rpeer[0] * (1 - t) + rpeer[1] * t
    mine = (
        first,
        pl.ds(pl.multiple_of(h * hd, hd), hd),
    )
    last = 3

    def unit_ref(u, slab):
        k = u % 2
        return gath.at[u // 2, slab, mine[u // 2], k * share : (k + 1) * share]

    def line(u, way, s, arrive=False):
        step = -1 if way == 0 else 1
        slab = f + step * s + (step if arrive else 0)
        ref = unit_ref(u, slab)
        dev = f + step if arrive else f - step
        to = f if arrive else dev
        slot = s if way == 0 else to + s
        return remote(ref, ref, sent.at[min(s, 1)], az_r.at[u, slot], (dev, r, t))

    def sends_line(way, s):
        return (f >= s) & (f < last) if way == 0 else (f + s <= last) & (f > 0)

    def gets_line(way, s):
        return f >= s + 1 if way == 0 else f + s + 1 <= last

    def carried(way):
        return f if way == 0 else last - f

    def share_slab(u, slab, slot):
        ref = unit_ref(u, slab)
        for q in (rpeer[2], rpeer[0], rpeer[1]) if u < 2 else (near,):
            remote(ref, ref, sent.at[2 if u < 2 else 9], aw_r.at[max(u - 1, 0), slot], (f, q, t)).start()

    def open_line(u, last_only=None):
        for way in range(2):
            go = sends_line(way, 0)
            if last_only is not None:
                go = go & ((carried(way) == 0) == last_only)

            @pl.when(go)
            def _():
                line(u, way, 0).start()

    def run_line(u, s):
        for way in range(2):
            @pl.when(gets_line(way, s))
            def _():
                line(u, way, s, True).wait_recv()
            if s < 2:
                @pl.when(sends_line(way, s + 1))
                def _():
                    line(u, way, s + 1).start()

            @pl.when(gets_line(way, s))
            def _():
                slab = f - 1 - s if way == 0 else f + 1 + s
                share_slab(u, slab, s if way == 0 else f + s)

    def swap_cot(p):
        ref = cot.at[p, t]
        return remote(ref, ref, sent.at[3], cx_r.at[p], (f, r, ot))

    def to_reps(u, k):
        j = 1 - x if k < 2 else x
        c = (0, 1, ot, t)[k]
        return remote(
            pb.at[u - 1, j, c], t1.at[u, r], sent.at[4], b1_r.at[u], (f, 2 * t + j, c)
        )

    def scatter_zs():
        for k in range(3):
            remote(
                zb.at[fpeer[k]], zt.at[k], sent.at[10], z_r.at[0], (fpeer[k], r, t)
            ).start()

    def to_owner(k):
        j = 1 - x if k < 2 else x
        c = (0, 1, ot, t)[k]
        return remote(yb.at[j, c], yt.at[r], sent.at[11], z_r.at[1], (f, 2 * t + j, c))

    def scatter_owners():
        settle(zt, z_r.at[0])
        total = zb[f].astype(jnp.float32)
        for k in range(3):
            total = total + zt[k].astype(jnp.float32)
        yb[...] = total.astype(jnp.bfloat16)
        for k in range(3):
            to_owner(k).start()

        @pl.when(t != y)
        def _():
            to_owner(3).start()

        @pl.when(t == y)
        def _():
            yt[r] = yb[x, t]

    def spread_own():
        @pl.when(t != y)
        def _():
            settle(yt, z_r.at[1])

        @pl.when(t == y)
        def _():
            settle(yt.at[:3], z_r.at[1])

        total = yt[0].astype(jnp.float32)
        for q in range(1, 4):
            total = total + yt[q].astype(jnp.float32)
        send_sums(0, total)

    def spread_sums():
        for k in (2, 1, 0):
            settle(ag.at[2, fpeer[k]], g_r.at[2, k])
            update_own(2, fpeer[k])

    def spread_zs():
        rows = rows_at(2, f)
        settle(full.at[1, :3, rows, :], z_r.at[2])
        for k in range(3):
            for q in rpeer:
                ref = full.at[1, q, rows, :]
                remote(ref, ref, sent.at[12], z_r.at[3], (fpeer[k], r, t)).start()

    def slab_dot(p, g, lanes):
        at = pl.ds(pl.multiple_of(g * depth, depth), depth)
        return jnp.dot(act[p, :, at], gath[p, g, :, lanes], preferred_element_type=jnp.float32)

    def lanes_of(us):
        return slice((us[0] % 2) * share, (us[-1] % 2 + 1) * share)

    def partial(p, us, slot):
        lanes = lanes_of(us)
        settle(gath.at[p, 0, : depth - (qd, hd)[p], lanes], aw_r.at[max(us[0] - 1, 0), slot])
        slab = jnp.where(slot < f, f - 1 - slot, slot + 1)
        return own[p, :, lanes] + slab_dot(p, slab, lanes)

    def prepare(p, us, slot):
        own[p, :, lanes_of(us)] = partial(p, us, slot)

    def project(p, us):
        part = partial(p, us, 2)
        part = part.astype(jnp.bfloat16)
        for i, u in reversed(tuple(enumerate(us))):
            for c in range(2):
                terms = lax.dot_general(
                    part[:, i * share : (i + 1) * share], cot[p, c], (((0,), (0,)), ((), ())),
                    preferred_element_type=jnp.float32,
                )
                for j in range(2):
                    block = terms[j * cut : (j + 1) * cut].astype(jnp.bfloat16)
                    if u > 0:
                        pb[u - 1, j, c] = block
                    else:
                        for g in range(4):
                            zb[g, j, c] = block[g * piece : (g + 1) * piece]
            if u > 0:
                scatter_reps(u)
            else:
                scatter_zs()

    def scatter_reps(u):
        for k in range(3):
            to_reps(u, k).start()

        @pl.when(t != y)
        def _():
            to_reps(u, 3).start()

        @pl.when(t == y)
        def _():
            t1[u, r] = pb[u - 1, x, t]

    def scatter_tokens(u):
        @pl.when(t != y)
        def _():
            settle(t1.at[u], b1_r.at[u])

        @pl.when(t == y)
        def _():
            settle(t1.at[u, :3], b1_r.at[u])

        total = t1[u, 0].astype(jnp.float32)
        for q in range(1, 4):
            total = total + t1[u, q].astype(jnp.float32)
        for g in range(4):
            sb[u, g] = total[g * piece : (g + 1) * piece].astype(jnp.bfloat16)
        for k in range(3):
            to_token(u, k).start()

    def to_token(u, k):
        return remote(
            sb.at[u, fpeer[k]], t2.at[u, k], sent.at[5], b2_r.at[u], (fpeer[k], r, t)
        )

    def rows_at(u, g):
        at = (u % 2) * cut + g * piece
        return pl.ds(pl.multiple_of(at, piece), piece)

    def to_dirs(u, g, k):
        ref = full.at[u // 2, r, rows_at(u, g), :]
        ss, rs = (sent.at[12], z_r.at[2]) if u == 2 else (sent.at[7], d_r.at[u // 2])
        return remote(ref, ref, ss, rs, (f, rpeer[k], t))

    def to_sums(u, k):
        return remote(
            ag.at[u, f], ag.at[u, f], sent.at[6], g_r.at[u, k], (fpeer[k], r, t)
        )

    def update_own(u, g):
        p, rows = u // 2, rows_at(u, g)
        new = BETA * old[p, rows, :] + (1.0 - BETA) * ag[u, g].astype(jnp.float32)
        mom[p, rows, :] = new
        full[p, r, rows, :] = new.astype(jnp.bfloat16)

    def update(u, g):
        update_own(u, g)
        for k in (2, 0, 1):
            to_dirs(u, g, k).start()

    def send_sums(u, total):
        ag[u, f] = total.astype(jnp.bfloat16)
        for k in range(3):
            to_sums(u, k).start()
        update(u, f)

    def gather_sums(u):
        total = sb[u, f].astype(jnp.float32)
        settle(t2.at[u], b2_r.at[u])
        for k in range(3):
            total = total + t2[u, k].astype(jnp.float32)
        send_sums(u, total)

    def gather_dirs(u):
        for k in (2, 1, 0):
            settle(ag.at[u, fpeer[k]], g_r.at[u, k])
            update(u, fpeer[k])

    others = [(q, s) for q in rpeer for s in (t, ot)] + [(r, ot)]
    me = 2 * r + t

    def to_norms(p, k):
        q, s = others[k]
        ref = nrm.at[p, me]
        return remote(ref, ref, sent.at[8], n_r.at[p], (f, q, s))

    def send_norms(p):
        sq = mom[p] * mom[p]
        lanes = sq[:, :128]
        for k in range(1, sq.shape[1] // 128):
            lanes = lanes + sq[:, k * 128 : (k + 1) * 128]
        acc = lanes[:8]
        for k in range(1, share // 8):
            acc = acc + lanes[k * 8 : (k + 1) * 8]
        nrm[p, me] = acc
        for k in range(7):
            to_norms(p, k).start()

    def sum_norms(p):
        settle(nrm.at[p, :7], n_r.at[p])
        acc = nrm[p, 0]
        for k in range(1, 8):
            acc = acc + nrm[p, k]
        total_sq[p] = acc

    def finish(p):
        sum_norms(p)
        if p == 0:
            settle(full.at[0, :3], d_r.at[0])
        else:
            settle(full.at[1, :3, : 3 * piece, :], z_r.at[3])
            settle(full.at[1, :3, :cut, :], d_r.at[1])

    open_line(0)
    open_line(1)
    loads[2].wait()
    deal(1, slice(None), base[1])
    open_line(2)
    open_line(3, True)
    loads[1].wait()
    for k in range(1, 4):
        rows = pl.ds(pl.multiple_of((r + k) % 4 * qd, qd), qd)
        deal(0, rows, base[0, rows, :])
    for p in range(2):
        loads[3 + p].wait()
        swap_cot(p).start()
    loads[7].wait()
    loads[8].wait()
    old[1] = mo[...].T
    for p in range(2):
        loads[5 + p].wait()
        own[p] = slab_dot(p, f, slice(None))
        settle(cot.at[p, ot], cx_r.at[p])
    run_line(0, 0)
    run_line(1, 0)
    open_line(3, False)
    run_line(0, 1)
    run_line(1, 1)
    run_line(2, 0)
    run_line(0, 2)
    run_line(1, 2)
    run_line(3, 0)
    run_line(2, 1)
    run_line(3, 1)
    prepare(0, (0, 1), 0)
    prepare(0, (0, 1), 1)
    run_line(2, 2)
    prepare(1, (2,), 0)
    run_line(3, 2)
    project(0, (0, 1))
    prepare(1, (2,), 1)
    project(1, (2,))
    prepare(1, (3,), 0)
    prepare(1, (3,), 1)
    project(1, (3,))
    scatter_tokens(1)
    scatter_tokens(2)
    scatter_owners()
    gather_sums(1)
    scatter_tokens(3)
    gather_sums(2)
    spread_own()
    gather_dirs(1)
    gather_sums(3)
    spread_zs()
    spread_sums()
    gather_dirs(0)
    send_norms(0)
    gather_dirs(3)
    send_norms(1)
    finish(0)
    finish(1)
    inner = (f > 0) & (f < last)

    @pl.when(inner)
    def _():
        settle(gath.at[0, :3, :, :share], sent.at[0])
        settle(gath.at[0, :3, : depth - qd], sent.at[1])

    @pl.when(jnp.logical_not(inner))
    def _():
        settle(gath.at[0, :3, :hd, :share], sent.at[0])

    for k in range(2):
        settle(gath.at[k, :3, : depth - (qd, hd)[k], :], sent.at[2 + 7 * k])
    settle(cot.at[0], sent.at[3])

    @pl.when(t != y)
    def _():
        settle(pb, sent.at[4])
        settle(yt, sent.at[11])

    @pl.when(t == y)
    def _():
        settle(pb.at[:, :, :, : 3 * piece], sent.at[4])
        settle(yt.at[:3], sent.at[11])

    settle(t2.at[:3], sent.at[5])
    settle(t2, sent.at[6])
    settle(full.at[:, :3, : 6 * piece], sent.at[7])
    settle(nrm.at[:, :7], sent.at[8])
    settle(zt, sent.at[10])
    settle(t2, sent.at[12])


def finish_kernel(
    entries, qb, ob, fq, fo, sq, qw, ow, mq, mo,
    qs_o, os_o, qn_o, on_o, qc_o, oc_o, mq_o, mo_o,
):
    def scale(p):
        rows = jnp.sum(sq[p], axis=0, keepdims=True)
        return lax.rsqrt(jnp.sum(rows, axis=1, keepdims=True) / entries + EPS)

    step = jnp.dot(qb[...], fq[0], preferred_element_type=jnp.float32) * scale(0)
    new = qw[...] - RATE * step
    qs_o[...] = step
    qn_o[...] = new
    qc_o[...] = new.astype(jnp.bfloat16)
    step = lax.dot_general(
        fo[0].T, ob[...], (((1,), (1,)), ((), ())), preferred_element_type=jnp.float32
    ) * scale(1)
    new = ow[...] - RATE * step
    os_o[...] = step
    on_o[...] = new
    oc_o[...] = new.astype(jnp.bfloat16)
    mq_o[...] = mq[0]
    mo_o[...] = mo[0].T


def on_device_fast(
    saved_input, query_cot, attn_out, out_cot, query_basis, output_basis,
    query_weight, output_weight, query_moment, output_moment,
):
    tokens, depth_all = saved_input.shape
    width = query_cot.shape[1]
    depth, rank = query_basis.shape
    share = rank // 4
    cut = share // 2
    piece = cut // 4
    entries = rank * width * lax.axis_size("tp")
    bf, f32 = jnp.bfloat16, jnp.float32
    any_spec = pl.BlockSpec(memory_space=pl.ANY)
    dma = pltpu.SemaphoreType.DMA
    ins = (
        saved_input, out_cot, query_cot, attn_out, query_basis, output_basis,
        query_moment, output_moment,
    )
    full, mom, norm = pl.pallas_call(
        exchange_kernel,
        out_shape=(
            jax.ShapeDtypeStruct((2, 4, share, width), bf),
            jax.ShapeDtypeStruct((2, share, width), f32),
            jax.ShapeDtypeStruct((2, 8, 128), f32),
        ),
        in_specs=[any_spec] * 8,
        out_specs=(pl.BlockSpec(memory_space=pltpu.VMEM),) * 3,
        scratch_shapes=[
            pltpu.VMEM((2, tokens, depth_all), bf),
            pltpu.VMEM((2, 2, tokens, width), bf),
            pltpu.VMEM((depth // 4, rank // 2), bf),
            pltpu.VMEM((2, depth, rank // 2), bf),
            pltpu.VMEM((2, share, width), f32),
            pltpu.VMEM((width, share), f32),
            pltpu.VMEM((2, 4, depth, 2 * share), bf),
            pltpu.VMEM((2, tokens, 2 * share), f32),
            pltpu.VMEM((UNITS - 1, 2, 2, cut, width), bf),
            pltpu.VMEM((UNITS, 4, cut, width), bf),
            pltpu.VMEM((UNITS, 4, piece, width), bf),
            pltpu.VMEM((UNITS, 3, piece, width), bf),
            pltpu.VMEM((UNITS, 4, piece, width), bf),
            pltpu.VMEM((2, 8, 8, 128), f32),
            pltpu.VMEM((4, 2, 2, piece, width), bf),
            pltpu.VMEM((3, 2, 2, piece, width), bf),
            pltpu.VMEM((2, 2, piece, width), bf),
            pltpu.VMEM((4, piece, width), bf),
            dma((9,)), dma((13,)), dma((2,)), dma((UNITS, 3)), dma((3, 3)), dma((UNITS,)),
            dma((UNITS,)), dma((UNITS, 3)), dma((2,)), dma((2,)), dma((4,)),
        ],
        compiler_params=pltpu.CompilerParams(
            collective_id=0, has_side_effects=True, vmem_limit_bytes=20 * 2**20
        ),
    )(*(pltpu.with_memory_space_constraint(a, pltpu.HBM) for a in ins))
    full = full.reshape(2, rank, width)
    n = 2
    rows = pl.BlockSpec((depth // n, rank), lambda i: (i, 0))
    whole = pl.BlockSpec((depth, rank), lambda i: (0, 0))
    wq = pl.BlockSpec((depth // n, width), lambda i: (i, 0))
    wo = pl.BlockSpec((width // n, depth), lambda i: (i, 0))
    mq = pl.BlockSpec((share // n, width), lambda i: (i, 0))
    mo = pl.BlockSpec((width // n, share), lambda i: (i, 0))
    sq, so = query_weight.shape, output_weight.shape
    return pl.pallas_call(
        functools.partial(finish_kernel, entries),
        grid=(n,),
        out_shape=tuple(
            jax.ShapeDtypeStruct(s, d)
            for s, d in (
                (sq, f32), (so, f32), (sq, f32), (so, f32), (sq, bf), (so, bf),
                (query_moment.shape, f32), (output_moment.shape, f32),
            )
        ),
        in_specs=[
            rows, whole,
            pl.BlockSpec((1, rank, width), lambda i: (0, 0, 0)),
            pl.BlockSpec((1, rank, width // n), lambda i: (1, 0, i)),
            pl.BlockSpec((2, 8, 128), lambda i: (0, 0, 0)),
            wq, wo,
            pl.BlockSpec((1, share // n, width), lambda i: (0, i, 0)),
            pl.BlockSpec((1, share, width // n), lambda i: (1, 0, i)),
        ],
        out_specs=(wq, wo, wq, wo, wq, wo, mq, mo),
        cost_estimate=pl.CostEstimate(
            flops=4 * depth * rank * width, bytes_accessed=20 * depth * width, transcendentals=0
        ),
        compiler_params=pltpu.CompilerParams(vmem_limit_bytes=20 * 2**20),
    )(query_basis, output_basis, full, full, norm, query_weight, output_weight, mom, mom)


def solution(mesh):
    small = dict(mesh.shape) == {"fs": 4, "rep": 4, "tp": 2}
    body = on_device_fast if small else on_device
    placed = (
        P(("fs", "rep"), None),
        P(("fs", "rep"), "tp"),
        P(("fs", "rep"), "tp"),
        P(("fs", "rep"), None),
        P("fs", None),
        P("fs", None),
        P("fs", "tp"),
        P("tp", "fs"),
        P("rep", "tp"),
        P("tp", "rep"),
    )
    return jax.shard_map(
        body,
        mesh=mesh,
        in_specs=placed,
        out_specs=(
            P("fs", "tp"),
            P("tp", "fs"),
            P("fs", "tp"),
            P("tp", "fs"),
            P("fs", "tp"),
            P("tp", "fs"),
            P("rep", "tp"),
            P("tp", "rep"),
        ),
        check_vma=False,
    )
```

```python
import functools

import jax
import jax.numpy as jnp
from jax import lax
from jax.experimental import pallas as pl
from jax.experimental.pallas import tpu as pltpu
from jax.sharding import PartitionSpec as P

BETA = 0.8
RATE = 0.2
EPS = 1e-06


def on_device(
    saved_input,
    query_cot,
    attn_out,
    out_cot,
    query_basis,
    output_basis,
    query_weight,
    output_weight,
    query_moment,
    output_moment,
):
    rank = query_basis.shape[1]
    grad_rows = lax.psum_scatter(
        jnp.dot(saved_input.T, query_cot, preferred_element_type=jnp.float32),
        "fs",
        scatter_dimension=0,
        tiled=True,
    )
    query_part = jnp.dot(
        query_basis.astype(jnp.float32).T, grad_rows, precision=lax.Precision.HIGHEST
    )
    cot_proj = jnp.dot(
        out_cot,
        lax.all_gather(output_basis, "fs", axis=0, tiled=True),
        preferred_element_type=jnp.float32,
    )
    output_part = jnp.dot(attn_out.astype(jnp.float32).T, cot_proj, precision=lax.Precision.HIGHEST)
    reps = lax.axis_size("rep")
    share = rank // reps
    query_terms, output_terms = (
        lax.all_to_all(
            query_part.astype(jnp.bfloat16), "rep", split_axis=0, concat_axis=0, tiled=True
        ).astype(query_part.dtype),
        lax.all_to_all(
            output_part.T.astype(jnp.bfloat16), "rep", split_axis=0, concat_axis=0, tiled=True
        ).astype(jnp.float32),
    )
    width = query_part.shape[1]
    query_local = jnp.sum(query_terms.reshape(reps, share, width), axis=0)
    output_local = jnp.sum(output_terms.reshape(reps, share, width), axis=0)
    query_share, output_flip = lax.psum((query_local, output_local), "fs")
    output_share = output_flip.T
    query_moment_new = BETA * query_moment + (1.0 - BETA) * query_share
    output_moment_new = BETA * output_moment + (1.0 - BETA) * output_share
    query_squares, output_squares = lax.psum(
        (
            jnp.sum(query_moment_new * query_moment_new),
            jnp.sum(output_moment_new * output_moment_new),
        ),
        ("rep", "tp"),
    )
    entries = rank * query_moment.shape[1] * lax.axis_size("tp")
    query_dir = (query_moment_new * lax.rsqrt(query_squares / entries + EPS)).astype(jnp.bfloat16)
    output_dir = (output_moment_new * lax.rsqrt(output_squares / entries + EPS)).astype(
        jnp.bfloat16
    )
    query_full, output_full = (
        lax.all_gather(query_dir, "rep", axis=0, tiled=True),
        lax.all_gather(output_dir, "rep", axis=1, tiled=True),
    )
    query_step = jnp.dot(query_basis, query_full, preferred_element_type=jnp.float32)
    output_step = jnp.dot(output_full, output_basis.T, preferred_element_type=jnp.float32)
    query_new = query_weight - RATE * query_step
    output_new = output_weight - RATE * output_step
    return (
        query_step,
        output_step,
        query_new,
        output_new,
        query_new.astype(jnp.bfloat16),
        output_new.astype(jnp.bfloat16),
        query_moment_new,
        output_moment_new,
    )


MESH = pl.DeviceIdType.MESH
UNITS = 4


def exchange_kernel(
    si_hbm, oc_hbm, qc_hbm, ao_hbm, qb_hbm, ob_hbm, mq_hbm, mo_hbm,
    full, mom, total_sq,
    act, cot, head, base, old, mo, gath, own, pb, t1, sb, t2, ag, nrm, zb, zt, yb, yt,
    load_sem, sent, cx_r, az_r, aw_r, b1_r, b2_r, g_r, n_r, d_r, z_r,
):
    f, r, t = lax.axis_index("fs"), lax.axis_index("rep"), lax.axis_index("tp")
    y, x = r // 2, r % 2
    ot = 1 - t
    fpeer = [3 - f, (f + 2) % 4, f + 1 - 2 * (f % 2)]
    rpeer = [2 * y + (1 - x), 2 * (1 - y) + x, 3 - r]
    depth, half = base.shape[1], base.shape[2]
    hd = depth // 2
    qd = depth // 4
    share = half // 2
    cut = share // 2
    piece = cut // 4

    cols = pl.ds(pl.multiple_of(t * half, half), half)
    first = pl.ds(pl.multiple_of(r * qd, qd), qd)
    loads = []
    for k, (src, dst) in enumerate((
        (qb_hbm.at[first, cols], head), (qb_hbm.at[:, cols], base.at[0]), (ob_hbm.at[:, cols], base.at[1]),
        (qc_hbm, cot.at[0, t]), (ao_hbm, cot.at[1, t]),
        (si_hbm, act.at[0]), (oc_hbm, act.at[1]),
        (mq_hbm, old.at[0]), (mo_hbm, mo),
    )):
        c = pltpu.make_async_copy(src, dst, load_sem.at[k])
        c.start()
        loads.append(c)

    barrier = pltpu.get_barrier_semaphore()
    for g in fpeer:
        pl.semaphore_signal(barrier, inc=1, device_id=(g, r, t), device_id_type=MESH)
    for q in rpeer:
        for s in (t, ot):
            pl.semaphore_signal(barrier, inc=1, device_id=(f, q, s), device_id_type=MESH)
    pl.semaphore_signal(barrier, inc=1, device_id=(f, r, ot), device_id_type=MESH)

    def deal(p, rows, block):
        lo, hi = block[:, :share], block[:, share:]
        gath[p, f, rows, :share] = jnp.concatenate([lo[:, :cut], hi[:, :cut]], axis=1)
        gath[p, f, rows, share:] = jnp.concatenate([lo[:, cut:], hi[:, cut:]], axis=1)

    loads[0].wait()
    deal(0, first, head[...])
    pl.semaphore_wait(barrier, 10)

    def remote(src, dst, ss, rs, dev):
        return pltpu.make_async_remote_copy(
            src_ref=src, dst_ref=dst, send_sem=ss, recv_sem=rs, device_id=dev, device_id_type=MESH
        )

    def settle(ref, sem):
        pltpu.make_async_copy(ref, ref, sem).wait()

    h = x * (1 - t) + y * t
    near = rpeer[0] * (1 - t) + rpeer[1] * t
    mine = (
        first,
        pl.ds(pl.multiple_of(h * hd, hd), hd),
    )
    last = 3

    def unit_ref(u, slab):
        k = u % 2
        return gath.at[u // 2, slab, mine[u // 2], k * share : (k + 1) * share]

    def line(u, way, s, arrive=False):
        step = -1 if way == 0 else 1
        slab = f + step * s + (step if arrive else 0)
        ref = unit_ref(u, slab)
        dev = f + step if arrive else f - step
        to = f if arrive else dev
        slot = s if way == 0 else to + s
        return remote(ref, ref, sent.at[min(s, 1)], az_r.at[u, slot], (dev, r, t))

    def sends_line(way, s):
        return (f >= s) & (f < last) if way == 0 else (f + s <= last) & (f > 0)

    def gets_line(way, s):
        return f >= s + 1 if way == 0 else f + s + 1 <= last

    def carried(way):
        return f if way == 0 else last - f

    def share_slab(u, slab, slot):
        ref = unit_ref(u, slab)
        for q in (rpeer[2], rpeer[0], rpeer[1]) if u < 2 else (near,):
            remote(ref, ref, sent.at[2 if u < 2 else 9], aw_r.at[max(u - 1, 0), slot], (f, q, t)).start()

    def open_line(u, last_only=None):
        for way in range(2):
            go = sends_line(way, 0)
            if last_only is not None:
                go = go & ((carried(way) == 0) == last_only)

            @pl.when(go)
            def _():
                line(u, way, 0).start()

    def run_line(u, s):
        for way in range(2):
            @pl.when(gets_line(way, s))
            def _():
                line(u, way, s, True).wait_recv()
            if s < 2:
                @pl.when(sends_line(way, s + 1))
                def _():
                    line(u, way, s + 1).start()

            @pl.when(gets_line(way, s))
            def _():
                slab = f - 1 - s if way == 0 else f + 1 + s
                share_slab(u, slab, s if way == 0 else f + s)

    def swap_cot(p):
        ref = cot.at[p, t]
        return remote(ref, ref, sent.at[3], cx_r.at[p], (f, r, ot))

    def to_reps(u, k):
        j = 1 - x if k < 2 else x
        c = (0, 1, ot, t)[k]
        return remote(
            pb.at[u - 1, j, c], t1.at[u, r], sent.at[4], b1_r.at[u], (f, 2 * t + j, c)
        )

    def scatter_zs():
        for k in range(3):
            remote(
                zb.at[fpeer[k]], zt.at[k], sent.at[10], z_r.at[0], (fpeer[k], r, t)
            ).start()

    def to_owner(k):
        j = 1 - x if k < 2 else x
        c = (0, 1, ot, t)[k]
        return remote(yb.at[j, c], yt.at[r], sent.at[11], z_r.at[1], (f, 2 * t + j, c))

    def scatter_owners():
        settle(zt, z_r.at[0])
        total = zb[f].astype(jnp.float32)
        for k in range(3):
            total = total + zt[k].astype(jnp.float32)
        yb[...] = total.astype(jnp.bfloat16)
        for k in range(3):
            to_owner(k).start()

        @pl.when(t != y)
        def _():
            to_owner(3).start()

        @pl.when(t == y)
        def _():
            yt[r] = yb[x, t]

    def spread_own():
        @pl.when(t != y)
        def _():
            settle(yt, z_r.at[1])

        @pl.when(t == y)
        def _():
            settle(yt.at[:3], z_r.at[1])

        total = yt[0].astype(jnp.float32)
        for q in range(1, 4):
            total = total + yt[q].astype(jnp.float32)
        send_sums(0, total)

    def spread_sums():
        for k in (2, 1, 0):
            settle(ag.at[2, fpeer[k]], g_r.at[2, k])
            update_own(2, fpeer[k])

    def spread_zs():
        rows = rows_at(2, f)
        settle(full.at[1, :3, rows, :], z_r.at[2])
        for k in range(3):
            for q in rpeer:
                ref = full.at[1, q, rows, :]
                remote(ref, ref, sent.at[12], z_r.at[3], (fpeer[k], r, t)).start()

    def slab_dot(p, g, lanes):
        at = pl.ds(pl.multiple_of(g * depth, depth), depth)
        return jnp.dot(act[p, :, at], gath[p, g, :, lanes], preferred_element_type=jnp.float32)

    def lanes_of(us):
        return slice((us[0] % 2) * share, (us[-1] % 2 + 1) * share)

    def partial(p, us, slot):
        lanes = lanes_of(us)
        settle(gath.at[p, 0, : depth - (qd, hd)[p], lanes], aw_r.at[max(us[0] - 1, 0), slot])
        slab = jnp.where(slot < f, f - 1 - slot, slot + 1)
        return own[p, :, lanes] + slab_dot(p, slab, lanes)

    def prepare(p, us, slot):
        own[p, :, lanes_of(us)] = partial(p, us, slot)

    def project(p, us, between=None):
        part = partial(p, us, 2)
        part = part.astype(jnp.bfloat16)
        for i, u in reversed(tuple(enumerate(us))):
            for c in range(2):
                terms = lax.dot_general(
                    part[:, i * share : (i + 1) * share], cot[p, c], (((0,), (0,)), ((), ())),
                    preferred_element_type=jnp.float32,
                )
                for j in range(2):
                    block = terms[j * cut : (j + 1) * cut].astype(jnp.bfloat16)
                    if u > 0:
                        pb[u - 1, j, c] = block
                    else:
                        for g in range(4):
                            zb[g, j, c] = block[g * piece : (g + 1) * piece]
            if between is not None and u == us[-1]:
                between()
            if u > 0:
                scatter_reps(u)
            else:
                scatter_zs()

    def scatter_reps(u):
        for k in range(3):
            to_reps(u, k).start()

        @pl.when(t != y)
        def _():
            to_reps(u, 3).start()

        @pl.when(t == y)
        def _():
            t1[u, r] = pb[u - 1, x, t]

    def scatter_tokens(u):
        @pl.when(t != y)
        def _():
            settle(t1.at[u], b1_r.at[u])

        @pl.when(t == y)
        def _():
            settle(t1.at[u, :3], b1_r.at[u])

        total = t1[u, 0].astype(jnp.float32)
        for q in range(1, 4):
            total = total + t1[u, q].astype(jnp.float32)
        for g in range(4):
            sb[u, g] = total[g * piece : (g + 1) * piece].astype(jnp.bfloat16)
        for k in range(3):
            to_token(u, k).start()

    def to_token(u, k):
        return remote(
            sb.at[u, fpeer[k]], t2.at[u, k], sent.at[5], b2_r.at[u], (fpeer[k], r, t)
        )

    def rows_at(u, g):
        at = (u % 2) * cut + g * piece
        return pl.ds(pl.multiple_of(at, piece), piece)

    def to_dirs(u, g, k):
        ref = full.at[u // 2, r, rows_at(u, g), :]
        ss, rs = (sent.at[12], z_r.at[2]) if u == 2 else (sent.at[7], d_r.at[u // 2])
        return remote(ref, ref, ss, rs, (f, rpeer[k], t))

    def to_sums(u, k):
        return remote(
            ag.at[u, f], ag.at[u, f], sent.at[6], g_r.at[u, k], (fpeer[k], r, t)
        )

    def update_own(u, g):
        p, rows = u // 2, rows_at(u, g)
        new = BETA * old[p, rows, :] + (1.0 - BETA) * ag[u, g].astype(jnp.float32)
        mom[p, rows, :] = new
        full[p, r, rows, :] = new.astype(jnp.bfloat16)

    def update(u, g):
        update_own(u, g)
        for k in (2, 0, 1):
            to_dirs(u, g, k).start()

    def send_sums(u, total):
        ag[u, f] = total.astype(jnp.bfloat16)
        for k in range(3):
            to_sums(u, k).start()
        update(u, f)

    def gather_sums(u):
        total = sb[u, f].astype(jnp.float32)
        settle(t2.at[u], b2_r.at[u])
        for k in range(3):
            total = total + t2[u, k].astype(jnp.float32)
        send_sums(u, total)

    def gather_dirs(u):
        for k in (2, 1, 0):
            settle(ag.at[u, fpeer[k]], g_r.at[u, k])
            update(u, fpeer[k])

    others = [(q, s) for q in rpeer for s in (t, ot)] + [(r, ot)]
    me = 2 * r + t

    def to_norms(p, k):
        q, s = others[k]
        ref = nrm.at[p, me]
        return remote(ref, ref, sent.at[8], n_r.at[p], (f, q, s))

    def send_norms(p):
        sq = mom[p] * mom[p]
        lanes = sq[:, :128]
        for k in range(1, sq.shape[1] // 128):
            lanes = lanes + sq[:, k * 128 : (k + 1) * 128]
        acc = lanes[:8]
        for k in range(1, share // 8):
            acc = acc + lanes[k * 8 : (k + 1) * 8]
        nrm[p, me] = acc
        for k in range(7):
            to_norms(p, k).start()

    def sum_norms(p):
        settle(nrm.at[p, :7], n_r.at[p])
        acc = nrm[p, 0]
        for k in range(1, 8):
            acc = acc + nrm[p, k]
        total_sq[p] = acc

    def finish(p):
        sum_norms(p)
        if p == 0:
            settle(full.at[0, :3], d_r.at[0])
        else:
            settle(full.at[1, :3, : 3 * piece, :], z_r.at[3])
            settle(full.at[1, :3, :cut, :], d_r.at[1])

    open_line(0)
    open_line(1)
    loads[2].wait()
    deal(1, slice(None), base[1])
    open_line(2)
    open_line(3, True)
    loads[1].wait()
    for k in range(1, 4):
        rows = pl.ds(pl.multiple_of((r + k) % 4 * qd, qd), qd)
        deal(0, rows, base[0, rows, :])
    for p in range(2):
        loads[3 + p].wait()
        swap_cot(p).start()
    loads[7].wait()
    loads[8].wait()
    old[1] = mo[...].T
    for p in range(2):
        loads[5 + p].wait()
        own[p] = slab_dot(p, f, slice(None))
        settle(cot.at[p, ot], cx_r.at[p])
    run_line(0, 0)
    run_line(1, 0)
    open_line(3, False)
    run_line(0, 1)
    run_line(1, 1)
    run_line(2, 0)
    run_line(0, 2)
    run_line(1, 2)
    run_line(3, 0)
    run_line(2, 1)
    run_line(3, 1)
    prepare(0, (0, 1), 0)
    prepare(0, (0, 1), 1)
    run_line(2, 2)
    project(0, (0, 1), lambda: run_line(3, 2))
    prepare(1, (2,), 0)
    prepare(1, (2,), 1)
    project(1, (2,))
    prepare(1, (3,), 0)
    prepare(1, (3,), 1)
    project(1, (3,))
    scatter_tokens(1)
    scatter_tokens(2)
    scatter_owners()
    gather_sums(1)
    scatter_tokens(3)
    gather_sums(2)
    spread_own()
    gather_dirs(1)
    gather_sums(3)
    spread_zs()
    spread_sums()
    gather_dirs(0)
    send_norms(0)
    gather_dirs(3)
    send_norms(1)
    finish(0)
    finish(1)
    inner = (f > 0) & (f < last)

    @pl.when(inner)
    def _():
        settle(gath.at[0, :3, :, :share], sent.at[0])
        settle(gath.at[0, :3, : depth - qd], sent.at[1])

    @pl.when(jnp.logical_not(inner))
    def _():
        settle(gath.at[0, :3, :hd, :share], sent.at[0])

    for k in range(2):
        settle(gath.at[k, :3, : depth - (qd, hd)[k], :], sent.at[2 + 7 * k])
    settle(cot.at[0], sent.at[3])

    @pl.when(t != y)
    def _():
        settle(pb, sent.at[4])
        settle(yt, sent.at[11])

    @pl.when(t == y)
    def _():
        settle(pb.at[:, :, :, : 3 * piece], sent.at[4])
        settle(yt.at[:3], sent.at[11])

    settle(t2.at[:3], sent.at[5])
    settle(t2, sent.at[6])
    settle(full.at[:, :3, : 6 * piece], sent.at[7])
    settle(nrm.at[:, :7], sent.at[8])
    settle(zt, sent.at[10])
    settle(t2, sent.at[12])


def finish_kernel(
    entries, qb, ob, fq, fo, sq, qw, ow, mq, mo,
    qs_o, os_o, qn_o, on_o, qc_o, oc_o, mq_o, mo_o,
):
    def scale(p):
        rows = jnp.sum(sq[p], axis=0, keepdims=True)
        return lax.rsqrt(jnp.sum(rows, axis=1, keepdims=True) / entries + EPS)

    step = jnp.dot(qb[...], fq[0], preferred_element_type=jnp.float32) * scale(0)
    new = qw[...] - RATE * step
    qs_o[...] = step
    qn_o[...] = new
    qc_o[...] = new.astype(jnp.bfloat16)
    step = lax.dot_general(
        fo[0].T, ob[...], (((1,), (1,)), ((), ())), preferred_element_type=jnp.float32
    ) * scale(1)
    new = ow[...] - RATE * step
    os_o[...] = step
    on_o[...] = new
    oc_o[...] = new.astype(jnp.bfloat16)
    mq_o[...] = mq[0]
    mo_o[...] = mo[0].T


def on_device_fast(
    saved_input, query_cot, attn_out, out_cot, query_basis, output_basis,
    query_weight, output_weight, query_moment, output_moment,
):
    tokens, depth_all = saved_input.shape
    width = query_cot.shape[1]
    depth, rank = query_basis.shape
    share = rank // 4
    cut = share // 2
    piece = cut // 4
    entries = rank * width * lax.axis_size("tp")
    bf, f32 = jnp.bfloat16, jnp.float32
    any_spec = pl.BlockSpec(memory_space=pl.ANY)
    dma = pltpu.SemaphoreType.DMA
    ins = (
        saved_input, out_cot, query_cot, attn_out, query_basis, output_basis,
        query_moment, output_moment,
    )
    full, mom, norm = pl.pallas_call(
        exchange_kernel,
        out_shape=(
            jax.ShapeDtypeStruct((2, 4, share, width), bf),
            jax.ShapeDtypeStruct((2, share, width), f32),
            jax.ShapeDtypeStruct((2, 8, 128), f32),
        ),
        in_specs=[any_spec] * 8,
        out_specs=(pl.BlockSpec(memory_space=pltpu.VMEM),) * 3,
        scratch_shapes=[
            pltpu.VMEM((2, tokens, depth_all), bf),
            pltpu.VMEM((2, 2, tokens, width), bf),
            pltpu.VMEM((depth // 4, rank // 2), bf),
            pltpu.VMEM((2, depth, rank // 2), bf),
            pltpu.VMEM((2, share, width), f32),
            pltpu.VMEM((width, share), f32),
            pltpu.VMEM((2, 4, depth, 2 * share), bf),
            pltpu.VMEM((2, tokens, 2 * share), f32),
            pltpu.VMEM((UNITS - 1, 2, 2, cut, width), bf),
            pltpu.VMEM((UNITS, 4, cut, width), bf),
            pltpu.VMEM((UNITS, 4, piece, width), bf),
            pltpu.VMEM((UNITS, 3, piece, width), bf),
            pltpu.VMEM((UNITS, 4, piece, width), bf),
            pltpu.VMEM((2, 8, 8, 128), f32),
            pltpu.VMEM((4, 2, 2, piece, width), bf),
            pltpu.VMEM((3, 2, 2, piece, width), bf),
            pltpu.VMEM((2, 2, piece, width), bf),
            pltpu.VMEM((4, piece, width), bf),
            dma((9,)), dma((13,)), dma((2,)), dma((UNITS, 3)), dma((3, 3)), dma((UNITS,)),
            dma((UNITS,)), dma((UNITS, 3)), dma((2,)), dma((2,)), dma((4,)),
        ],
        compiler_params=pltpu.CompilerParams(
            collective_id=0, has_side_effects=True, vmem_limit_bytes=20 * 2**20
        ),
    )(*(pltpu.with_memory_space_constraint(a, pltpu.HBM) for a in ins))
    full = full.reshape(2, rank, width)
    n = 2
    rows = pl.BlockSpec((depth // n, rank), lambda i: (i, 0))
    whole = pl.BlockSpec((depth, rank), lambda i: (0, 0))
    wq = pl.BlockSpec((depth // n, width), lambda i: (i, 0))
    wo = pl.BlockSpec((width // n, depth), lambda i: (i, 0))
    mq = pl.BlockSpec((share // n, width), lambda i: (i, 0))
    mo = pl.BlockSpec((width // n, share), lambda i: (i, 0))
    sq, so = query_weight.shape, output_weight.shape
    return pl.pallas_call(
        functools.partial(finish_kernel, entries),
        grid=(n,),
        out_shape=tuple(
            jax.ShapeDtypeStruct(s, d)
            for s, d in (
                (sq, f32), (so, f32), (sq, f32), (so, f32), (sq, bf), (so, bf),
                (query_moment.shape, f32), (output_moment.shape, f32),
            )
        ),
        in_specs=[
            rows, whole,
            pl.BlockSpec((1, rank, width), lambda i: (0, 0, 0)),
            pl.BlockSpec((1, rank, width // n), lambda i: (1, 0, i)),
            pl.BlockSpec((2, 8, 128), lambda i: (0, 0, 0)),
            wq, wo,
            pl.BlockSpec((1, share // n, width), lambda i: (0, i, 0)),
            pl.BlockSpec((1, share, width // n), lambda i: (1, 0, i)),
        ],
        out_specs=(wq, wo, wq, wo, wq, wo, mq, mo),
        cost_estimate=pl.CostEstimate(
            flops=4 * depth * rank * width, bytes_accessed=20 * depth * width, transcendentals=0
        ),
        compiler_params=pltpu.CompilerParams(vmem_limit_bytes=20 * 2**20),
    )(query_basis, output_basis, full, full, norm, query_weight, output_weight, mom, mom)


def solution(mesh):
    small = dict(mesh.shape) == {"fs": 4, "rep": 4, "tp": 2}
    body = on_device_fast if small else on_device
    placed = (
        P(("fs", "rep"), None),
        P(("fs", "rep"), "tp"),
        P(("fs", "rep"), "tp"),
        P(("fs", "rep"), None),
        P("fs", None),
        P("fs", None),
        P("fs", "tp"),
        P("tp", "fs"),
        P("rep", "tp"),
        P("tp", "rep"),
    )
    return jax.shard_map(
        body,
        mesh=mesh,
        in_specs=placed,
        out_specs=(
            P("fs", "tp"),
            P("tp", "fs"),
            P("fs", "tp"),
            P("tp", "fs"),
            P("fs", "tp"),
            P("tp", "fs"),
            P("rep", "tp"),
            P("tp", "rep"),
        ),
        check_vma=False,
    )
```

```python
import functools

import jax
import jax.numpy as jnp
from jax import lax
from jax.experimental import pallas as pl
from jax.experimental.pallas import tpu as pltpu
from jax.sharding import PartitionSpec as P

BETA = 0.8
RATE = 0.2
EPS = 1e-06


def on_device(
    saved_input,
    query_cot,
    attn_out,
    out_cot,
    query_basis,
    output_basis,
    query_weight,
    output_weight,
    query_moment,
    output_moment,
):
    rank = query_basis.shape[1]
    grad_rows = lax.psum_scatter(
        jnp.dot(saved_input.T, query_cot, preferred_element_type=jnp.float32),
        "fs",
        scatter_dimension=0,
        tiled=True,
    )
    query_part = jnp.dot(
        query_basis.astype(jnp.float32).T, grad_rows, precision=lax.Precision.HIGHEST
    )
    cot_proj = jnp.dot(
        out_cot,
        lax.all_gather(output_basis, "fs", axis=0, tiled=True),
        preferred_element_type=jnp.float32,
    )
    output_part = jnp.dot(attn_out.astype(jnp.float32).T, cot_proj, precision=lax.Precision.HIGHEST)
    reps = lax.axis_size("rep")
    share = rank // reps
    query_terms, output_terms = (
        lax.all_to_all(
            query_part.astype(jnp.bfloat16), "rep", split_axis=0, concat_axis=0, tiled=True
        ).astype(query_part.dtype),
        lax.all_to_all(
            output_part.T.astype(jnp.bfloat16), "rep", split_axis=0, concat_axis=0, tiled=True
        ).astype(jnp.float32),
    )
    width = query_part.shape[1]
    query_local = jnp.sum(query_terms.reshape(reps, share, width), axis=0)
    output_local = jnp.sum(output_terms.reshape(reps, share, width), axis=0)
    query_share, output_flip = lax.psum((query_local, output_local), "fs")
    output_share = output_flip.T
    query_moment_new = BETA * query_moment + (1.0 - BETA) * query_share
    output_moment_new = BETA * output_moment + (1.0 - BETA) * output_share
    query_squares, output_squares = lax.psum(
        (
            jnp.sum(query_moment_new * query_moment_new),
            jnp.sum(output_moment_new * output_moment_new),
        ),
        ("rep", "tp"),
    )
    entries = rank * query_moment.shape[1] * lax.axis_size("tp")
    query_dir = (query_moment_new * lax.rsqrt(query_squares / entries + EPS)).astype(jnp.bfloat16)
    output_dir = (output_moment_new * lax.rsqrt(output_squares / entries + EPS)).astype(
        jnp.bfloat16
    )
    query_full, output_full = (
        lax.all_gather(query_dir, "rep", axis=0, tiled=True),
        lax.all_gather(output_dir, "rep", axis=1, tiled=True),
    )
    query_step = jnp.dot(query_basis, query_full, preferred_element_type=jnp.float32)
    output_step = jnp.dot(output_full, output_basis.T, preferred_element_type=jnp.float32)
    query_new = query_weight - RATE * query_step
    output_new = output_weight - RATE * output_step
    return (
        query_step,
        output_step,
        query_new,
        output_new,
        query_new.astype(jnp.bfloat16),
        output_new.astype(jnp.bfloat16),
        query_moment_new,
        output_moment_new,
    )


MESH = pl.DeviceIdType.MESH
UNITS = 4


def exchange_kernel(
    si_hbm, oc_hbm, qc_hbm, ao_hbm, qb_hbm, ob_hbm, mq_hbm, mo_hbm,
    full, mom, total_sq,
    act, cot, head, base, old, mo, gath, own, pb, t1, sb, t2, ag, nrm, zb, zt, yb, yt,
    load_sem, sent, cx_r, az_r, aw_r, b1_r, b2_r, g_r, n_r, d_r, z_r,
):
    f, r, t = lax.axis_index("fs"), lax.axis_index("rep"), lax.axis_index("tp")
    y, x = r // 2, r % 2
    ot = 1 - t
    fpeer = [3 - f, (f + 2) % 4, f + 1 - 2 * (f % 2)]
    rpeer = [2 * y + (1 - x), 2 * (1 - y) + x, 3 - r]
    depth, half = base.shape[1], base.shape[2]
    hd = depth // 2
    qd = depth // 4
    share = half // 2
    cut = share // 2
    piece = cut // 4

    cols = pl.ds(pl.multiple_of(t * half, half), half)
    first = pl.ds(pl.multiple_of(r * qd, qd), qd)
    loads = []
    for k, (src, dst) in enumerate((
        (qb_hbm.at[first, cols], head), (qb_hbm.at[:, cols], base.at[0]), (ob_hbm.at[:, cols], base.at[1]),
        (qc_hbm, cot.at[0, t]), (ao_hbm, cot.at[1, t]),
        (si_hbm, act.at[0]), (oc_hbm, act.at[1]),
        (mq_hbm, old.at[0]), (mo_hbm, mo),
    )):
        c = pltpu.make_async_copy(src, dst, load_sem.at[k])
        c.start()
        loads.append(c)

    barrier = pltpu.get_barrier_semaphore()
    for g in fpeer:
        pl.semaphore_signal(barrier, inc=1, device_id=(g, r, t), device_id_type=MESH)
    for q in rpeer:
        for s in (t, ot):
            pl.semaphore_signal(barrier, inc=1, device_id=(f, q, s), device_id_type=MESH)
    pl.semaphore_signal(barrier, inc=1, device_id=(f, r, ot), device_id_type=MESH)

    def deal(p, rows, block):
        lo, hi = block[:, :share], block[:, share:]
        gath[p, f, rows, :share] = jnp.concatenate([lo[:, :cut], hi[:, :cut]], axis=1)
        gath[p, f, rows, share:] = jnp.concatenate([lo[:, cut:], hi[:, cut:]], axis=1)

    loads[0].wait()
    deal(0, first, head[...])
    pl.semaphore_wait(barrier, 10)

    def remote(src, dst, ss, rs, dev):
        return pltpu.make_async_remote_copy(
            src_ref=src, dst_ref=dst, send_sem=ss, recv_sem=rs, device_id=dev, device_id_type=MESH
        )

    def settle(ref, sem):
        pltpu.make_async_copy(ref, ref, sem).wait()

    h = x * (1 - t) + y * t
    near = rpeer[0] * (1 - t) + rpeer[1] * t
    mine = (
        first,
        pl.ds(pl.multiple_of(h * hd, hd), hd),
    )
    last = 3

    def unit_ref(u, slab):
        k = u % 2
        return gath.at[u // 2, slab, mine[u // 2], k * share : (k + 1) * share]

    def line(u, way, s, arrive=False):
        step = -1 if way == 0 else 1
        slab = f + step * s + (step if arrive else 0)
        ref = unit_ref(u, slab)
        dev = f + step if arrive else f - step
        to = f if arrive else dev
        slot = s if way == 0 else to + s
        return remote(ref, ref, sent.at[min(s, 1)], az_r.at[u, slot], (dev, r, t))

    def sends_line(way, s):
        return (f >= s) & (f < last) if way == 0 else (f + s <= last) & (f > 0)

    def gets_line(way, s):
        return f >= s + 1 if way == 0 else f + s + 1 <= last

    def carried(way):
        return f if way == 0 else last - f

    def share_slab(u, slab, slot):
        ref = unit_ref(u, slab)
        for q in (rpeer[2], rpeer[0], rpeer[1]) if u < 2 else (near,):
            remote(ref, ref, sent.at[2 if u < 2 else 9], aw_r.at[u, slot], (f, q, t)).start()

    def open_line(u, last_only=None):
        for way in range(2):
            go = sends_line(way, 0)
            if last_only is not None:
                go = go & ((carried(way) == 0) == last_only)

            @pl.when(go)
            def _():
                line(u, way, 0).start()

    def run_line(u, s):
        for way in range(2):
            @pl.when(gets_line(way, s))
            def _():
                line(u, way, s, True).wait_recv()
            if s < 2:
                @pl.when(sends_line(way, s + 1))
                def _():
                    line(u, way, s + 1).start()

            @pl.when(gets_line(way, s))
            def _():
                slab = f - 1 - s if way == 0 else f + 1 + s
                share_slab(u, slab, s if way == 0 else f + s)

    def swap_cot(p):
        ref = cot.at[p, t]
        return remote(ref, ref, sent.at[3], cx_r.at[p], (f, r, ot))

    def to_reps(u, k):
        j = 1 - x if k < 2 else x
        c = (0, 1, ot, t)[k]
        return remote(
            pb.at[u - 1, j, c], t1.at[u, r], sent.at[4], b1_r.at[u], (f, 2 * t + j, c)
        )

    def scatter_zs():
        for k in range(3):
            remote(
                zb.at[fpeer[k]], zt.at[k], sent.at[10], z_r.at[0], (fpeer[k], r, t)
            ).start()

    def to_owner(k):
        j = 1 - x if k < 2 else x
        c = (0, 1, ot, t)[k]
        return remote(yb.at[j, c], yt.at[r], sent.at[11], z_r.at[1], (f, 2 * t + j, c))

    def scatter_owners():
        settle(zt, z_r.at[0])
        total = zb[f].astype(jnp.float32)
        for k in range(3):
            total = total + zt[k].astype(jnp.float32)
        yb[...] = total.astype(jnp.bfloat16)
        for k in range(3):
            to_owner(k).start()

        @pl.when(t != y)
        def _():
            to_owner(3).start()

        @pl.when(t == y)
        def _():
            yt[r] = yb[x, t]

    def spread_own():
        @pl.when(t != y)
        def _():
            settle(yt, z_r.at[1])

        @pl.when(t == y)
        def _():
            settle(yt.at[:3], z_r.at[1])

        total = yt[0].astype(jnp.float32)
        for q in range(1, 4):
            total = total + yt[q].astype(jnp.float32)
        send_sums(0, total)

    def spread_sums():
        for k in (2, 1, 0):
            settle(ag.at[2, fpeer[k]], g_r.at[2, k])
            update_own(2, fpeer[k])

    def spread_zs():
        rows = rows_at(2, f)
        for j in range(3):
            ref = full.at[1, rpeer[j], rows, :]
            settle(ref, z_r.at[2 + j])
            for k in range(3):
                remote(ref, ref, sent.at[12], z_r.at[5], (fpeer[k], r, t)).start()

    def slab_dot(p, g, lanes):
        at = pl.ds(pl.multiple_of(g * depth, depth), depth)
        return jnp.dot(act[p, :, at], gath[p, g, :, lanes], preferred_element_type=jnp.float32)

    def lanes_of(us):
        return slice((us[0] % 2) * share, (us[-1] % 2 + 1) * share)

    def partial(p, us, slot):
        lanes = lanes_of(us)
        settle(gath.at[p, 0, : depth - (qd, hd)[p], lanes], aw_r.at[us[0], slot])
        slab = jnp.where(slot < f, f - 1 - slot, slot + 1)
        return own[p, :, lanes] + slab_dot(p, slab, lanes)

    def prepare(p, us, slot):
        own[p, :, lanes_of(us)] = partial(p, us, slot)

    def project(p, us):
        part = partial(p, us, 2)
        part = part.astype(jnp.bfloat16)
        for i, u in reversed(tuple(enumerate(us))):
            for c in range(2):
                terms = lax.dot_general(
                    part[:, i * share : (i + 1) * share], cot[p, c], (((0,), (0,)), ((), ())),
                    preferred_element_type=jnp.float32,
                )
                for j in range(2):
                    block = terms[j * cut : (j + 1) * cut].astype(jnp.bfloat16)
                    if u > 0:
                        pb[u - 1, j, c] = block
                    else:
                        for g in range(4):
                            zb[g, j, c] = block[g * piece : (g + 1) * piece]
            if u > 0:
                scatter_reps(u)
            else:
                scatter_zs()

    def scatter_reps(u):
        for k in range(3):
            to_reps(u, k).start()

        @pl.when(t != y)
        def _():
            to_reps(u, 3).start()

        @pl.when(t == y)
        def _():
            t1[u, r] = pb[u - 1, x, t]

    def scatter_tokens(u):
        @pl.when(t != y)
        def _():
            settle(t1.at[u], b1_r.at[u])

        @pl.when(t == y)
        def _():
            settle(t1.at[u, :3], b1_r.at[u])

        total = t1[u, 0].astype(jnp.float32)
        for q in range(1, 4):
            total = total + t1[u, q].astype(jnp.float32)
        for g in range(4):
            sb[u, g] = total[g * piece : (g + 1) * piece].astype(jnp.bfloat16)
        for k in range(3):
            to_token(u, k).start()

    def to_token(u, k):
        return remote(
            sb.at[u, fpeer[k]], t2.at[u, k], sent.at[5], b2_r.at[u], (fpeer[k], r, t)
        )

    def rows_at(u, g):
        at = (u % 2) * cut + g * piece
        return pl.ds(pl.multiple_of(at, piece), piece)

    def to_dirs(u, g, k):
        ref = full.at[u // 2, r, rows_at(u, g), :]
        ss, rs = (sent.at[12], z_r.at[2 + k]) if u == 2 else (sent.at[7], d_r.at[u // 2])
        return remote(ref, ref, ss, rs, (f, rpeer[k], t))

    def to_sums(u, k):
        return remote(
            ag.at[u, f], ag.at[u, f], sent.at[6], g_r.at[u, k], (fpeer[k], r, t)
        )

    def update_own(u, g):
        p, rows = u // 2, rows_at(u, g)
        new = BETA * old[p, rows, :] + (1.0 - BETA) * ag[u, g].astype(jnp.float32)
        mom[p, rows, :] = new
        full[p, r, rows, :] = new.astype(jnp.bfloat16)

    def update(u, g):
        update_own(u, g)
        for k in (2, 0, 1):
            to_dirs(u, g, k).start()

    def send_sums(u, total):
        ag[u, f] = total.astype(jnp.bfloat16)
        for k in range(3):
            to_sums(u, k).start()
        update(u, f)

    def gather_sums(u):
        total = sb[u, f].astype(jnp.float32)
        settle(t2.at[u], b2_r.at[u])
        for k in range(3):
            total = total + t2[u, k].astype(jnp.float32)
        send_sums(u, total)

    def gather_dirs(u):
        for k in (2, 1, 0):
            settle(ag.at[u, fpeer[k]], g_r.at[u, k])
            update(u, fpeer[k])

    others = [(q, s) for q in rpeer for s in (t, ot)] + [(r, ot)]
    me = 2 * r + t

    def to_norms(p, k):
        q, s = others[k]
        ref = nrm.at[p, me]
        return remote(ref, ref, sent.at[8], n_r.at[p], (f, q, s))

    def send_norms(p):
        sq = mom[p] * mom[p]
        lanes = sq[:, :128]
        for k in range(1, sq.shape[1] // 128):
            lanes = lanes + sq[:, k * 128 : (k + 1) * 128]
        acc = lanes[:8]
        for k in range(1, share // 8):
            acc = acc + lanes[k * 8 : (k + 1) * 8]
        nrm[p, me] = acc
        for k in range(7):
            to_norms(p, k).start()

    def sum_norms(p):
        settle(nrm.at[p, :7], n_r.at[p])
        acc = nrm[p, 0]
        for k in range(1, 8):
            acc = acc + nrm[p, k]
        total_sq[p] = acc

    def finish(p):
        sum_norms(p)
        if p == 0:
            settle(full.at[0, :3], d_r.at[0])
        else:
            settle(full.at[1, :3, : 3 * piece, :], z_r.at[5])
            settle(full.at[1, :3, :cut, :], d_r.at[1])

    open_line(1)
    open_line(0)
    loads[2].wait()
    deal(1, slice(None), base[1])
    open_line(2)
    open_line(3, True)
    loads[1].wait()
    for k in range(1, 4):
        rows = pl.ds(pl.multiple_of((r + k) % 4 * qd, qd), qd)
        deal(0, rows, base[0, rows, :])
    for p in range(2):
        loads[3 + p].wait()
        swap_cot(p).start()
    loads[7].wait()
    loads[8].wait()
    old[1] = mo[...].T
    for p in range(2):
        loads[5 + p].wait()
        own[p] = slab_dot(p, f, slice(None))
        settle(cot.at[p, ot], cx_r.at[p])
    run_line(1, 0)
    run_line(0, 0)
    open_line(3, False)
    run_line(1, 1)
    run_line(0, 1)
    run_line(2, 0)
    run_line(1, 2)
    run_line(0, 2)
    run_line(3, 0)
    run_line(2, 1)
    run_line(3, 1)
    prepare(0, (1,), 0)
    prepare(0, (0,), 0)
    prepare(0, (1,), 1)
    run_line(2, 2)
    prepare(0, (0,), 1)
    project(0, (1,))
    run_line(3, 2)
    project(0, (0,))
    prepare(1, (2,), 0)
    prepare(1, (2,), 1)
    project(1, (2,))
    prepare(1, (3,), 0)
    prepare(1, (3,), 1)
    project(1, (3,))
    scatter_tokens(1)
    scatter_owners()
    scatter_tokens(2)
    gather_sums(1)
    scatter_tokens(3)
    spread_own()
    gather_sums(2)
    gather_dirs(1)
    gather_sums(3)
    gather_dirs(0)
    send_norms(0)
    spread_zs()
    spread_sums()
    gather_dirs(3)
    send_norms(1)
    finish(0)
    finish(1)
    inner = (f > 0) & (f < last)

    @pl.when(inner)
    def _():
        settle(gath.at[0, :3, :, :share], sent.at[0])
        settle(gath.at[0, :3, : depth - qd], sent.at[1])

    @pl.when(jnp.logical_not(inner))
    def _():
        settle(gath.at[0, :3, :hd, :share], sent.at[0])

    for k in range(2):
        settle(gath.at[k, :3, : depth - (qd, hd)[k], :], sent.at[2 + 7 * k])
    settle(cot.at[0], sent.at[3])

    @pl.when(t != y)
    def _():
        settle(pb, sent.at[4])
        settle(yt, sent.at[11])

    @pl.when(t == y)
    def _():
        settle(pb.at[:, :, :, : 3 * piece], sent.at[4])
        settle(yt.at[:3], sent.at[11])

    settle(t2.at[:3], sent.at[5])
    settle(t2, sent.at[6])
    settle(full.at[:, :3, : 6 * piece], sent.at[7])
    settle(nrm.at[:, :7], sent.at[8])
    settle(zt, sent.at[10])
    settle(t2, sent.at[12])


def finish_kernel(
    entries, qb, ob, fq, fo, sq, qw, ow, mq, mo,
    qs_o, os_o, qn_o, on_o, qc_o, oc_o, mq_o, mo_o,
):
    def scale(p):
        rows = jnp.sum(sq[p], axis=0, keepdims=True)
        return lax.rsqrt(jnp.sum(rows, axis=1, keepdims=True) / entries + EPS)

    step = jnp.dot(qb[...], fq[0], preferred_element_type=jnp.float32) * scale(0)
    new = qw[...] - RATE * step
    qs_o[...] = step
    qn_o[...] = new
    qc_o[...] = new.astype(jnp.bfloat16)
    step = lax.dot_general(
        fo[0].T, ob[...], (((1,), (1,)), ((), ())), preferred_element_type=jnp.float32
    ) * scale(1)
    new = ow[...] - RATE * step
    os_o[...] = step
    on_o[...] = new
    oc_o[...] = new.astype(jnp.bfloat16)
    mq_o[...] = mq[0]
    mo_o[...] = mo[0].T


def on_device_fast(
    saved_input, query_cot, attn_out, out_cot, query_basis, output_basis,
    query_weight, output_weight, query_moment, output_moment,
):
    tokens, depth_all = saved_input.shape
    width = query_cot.shape[1]
    depth, rank = query_basis.shape
    share = rank // 4
    cut = share // 2
    piece = cut // 4
    entries = rank * width * lax.axis_size("tp")
    bf, f32 = jnp.bfloat16, jnp.float32
    any_spec = pl.BlockSpec(memory_space=pl.ANY)
    dma = pltpu.SemaphoreType.DMA
    ins = (
        saved_input, out_cot, query_cot, attn_out, query_basis, output_basis,
        query_moment, output_moment,
    )
    full, mom, norm = pl.pallas_call(
        exchange_kernel,
        out_shape=(
            jax.ShapeDtypeStruct((2, 4, share, width), bf),
            jax.ShapeDtypeStruct((2, share, width), f32),
            jax.ShapeDtypeStruct((2, 8, 128), f32),
        ),
        in_specs=[any_spec] * 8,
        out_specs=(pl.BlockSpec(memory_space=pltpu.VMEM),) * 3,
        scratch_shapes=[
            pltpu.VMEM((2, tokens, depth_all), bf),
            pltpu.VMEM((2, 2, tokens, width), bf),
            pltpu.VMEM((depth // 4, rank // 2), bf),
            pltpu.VMEM((2, depth, rank // 2), bf),
            pltpu.VMEM((2, share, width), f32),
            pltpu.VMEM((width, share), f32),
            pltpu.VMEM((2, 4, depth, 2 * share), bf),
            pltpu.VMEM((2, tokens, 2 * share), f32),
            pltpu.VMEM((UNITS - 1, 2, 2, cut, width), bf),
            pltpu.VMEM((UNITS, 4, cut, width), bf),
            pltpu.VMEM((UNITS, 4, piece, width), bf),
            pltpu.VMEM((UNITS, 3, piece, width), bf),
            pltpu.VMEM((UNITS, 4, piece, width), bf),
            pltpu.VMEM((2, 8, 8, 128), f32),
            pltpu.VMEM((4, 2, 2, piece, width), bf),
            pltpu.VMEM((3, 2, 2, piece, width), bf),
            pltpu.VMEM((2, 2, piece, width), bf),
            pltpu.VMEM((4, piece, width), bf),
            dma((9,)), dma((13,)), dma((2,)), dma((UNITS, 3)), dma((UNITS, 3)), dma((UNITS,)),
            dma((UNITS,)), dma((UNITS, 3)), dma((2,)), dma((2,)), dma((6,)),
        ],
        compiler_params=pltpu.CompilerParams(
            collective_id=0, has_side_effects=True, vmem_limit_bytes=20 * 2**20
        ),
    )(*(pltpu.with_memory_space_constraint(a, pltpu.HBM) for a in ins))
    full = full.reshape(2, rank, width)
    n = 2
    rows = pl.BlockSpec((depth // n, rank), lambda i: (i, 0))
    whole = pl.BlockSpec((depth, rank), lambda i: (0, 0))
    wq = pl.BlockSpec((depth // n, width), lambda i: (i, 0))
    wo = pl.BlockSpec((width // n, depth), lambda i: (i, 0))
    mq = pl.BlockSpec((share // n, width), lambda i: (i, 0))
    mo = pl.BlockSpec((width // n, share), lambda i: (i, 0))
    sq, so = query_weight.shape, output_weight.shape
    return pl.pallas_call(
        functools.partial(finish_kernel, entries),
        grid=(n,),
        out_shape=tuple(
            jax.ShapeDtypeStruct(s, d)
            for s, d in (
                (sq, f32), (so, f32), (sq, f32), (so, f32), (sq, bf), (so, bf),
                (query_moment.shape, f32), (output_moment.shape, f32),
            )
        ),
        in_specs=[
            rows, whole,
            pl.BlockSpec((1, rank, width), lambda i: (0, 0, 0)),
            pl.BlockSpec((1, rank, width // n), lambda i: (1, 0, i)),
            pl.BlockSpec((2, 8, 128), lambda i: (0, 0, 0)),
            wq, wo,
            pl.BlockSpec((1, share // n, width), lambda i: (0, i, 0)),
            pl.BlockSpec((1, share, width // n), lambda i: (1, 0, i)),
        ],
        out_specs=(wq, wo, wq, wo, wq, wo, mq, mo),
        cost_estimate=pl.CostEstimate(
            flops=4 * depth * rank * width, bytes_accessed=20 * depth * width, transcendentals=0
        ),
        compiler_params=pltpu.CompilerParams(vmem_limit_bytes=20 * 2**20),
    )(query_basis, output_basis, full, full, norm, query_weight, output_weight, mom, mom)


def solution(mesh):
    small = dict(mesh.shape) == {"fs": 4, "rep": 4, "tp": 2}
    body = on_device_fast if small else on_device
    placed = (
        P(("fs", "rep"), None),
        P(("fs", "rep"), "tp"),
        P(("fs", "rep"), "tp"),
        P(("fs", "rep"), None),
        P("fs", None),
        P("fs", None),
        P("fs", "tp"),
        P("tp", "fs"),
        P("rep", "tp"),
        P("tp", "rep"),
    )
    return jax.shard_map(
        body,
        mesh=mesh,
        in_specs=placed,
        out_specs=(
            P("fs", "tp"),
            P("tp", "fs"),
            P("fs", "tp"),
            P("tp", "fs"),
            P("fs", "tp"),
            P("tp", "fs"),
            P("rep", "tp"),
            P("tp", "rep"),
        ),
        check_vma=False,
    )
```

```python
import functools

import jax
import jax.numpy as jnp
from jax import lax
from jax.experimental import pallas as pl
from jax.experimental.pallas import tpu as pltpu
from jax.sharding import PartitionSpec as P

BETA = 0.8
RATE = 0.2
EPS = 1e-06


def on_device(
    saved_input,
    query_cot,
    attn_out,
    out_cot,
    query_basis,
    output_basis,
    query_weight,
    output_weight,
    query_moment,
    output_moment,
):
    rank = query_basis.shape[1]
    grad_rows = lax.psum_scatter(
        jnp.dot(saved_input.T, query_cot, preferred_element_type=jnp.float32),
        "fs",
        scatter_dimension=0,
        tiled=True,
    )
    query_part = jnp.dot(
        query_basis.astype(jnp.float32).T, grad_rows, precision=lax.Precision.HIGHEST
    )
    cot_proj = jnp.dot(
        out_cot,
        lax.all_gather(output_basis, "fs", axis=0, tiled=True),
        preferred_element_type=jnp.float32,
    )
    output_part = jnp.dot(attn_out.astype(jnp.float32).T, cot_proj, precision=lax.Precision.HIGHEST)
    reps = lax.axis_size("rep")
    share = rank // reps
    query_terms, output_terms = (
        lax.all_to_all(
            query_part.astype(jnp.bfloat16), "rep", split_axis=0, concat_axis=0, tiled=True
        ).astype(query_part.dtype),
        lax.all_to_all(
            output_part.T.astype(jnp.bfloat16), "rep", split_axis=0, concat_axis=0, tiled=True
        ).astype(jnp.float32),
    )
    width = query_part.shape[1]
    query_local = jnp.sum(query_terms.reshape(reps, share, width), axis=0)
    output_local = jnp.sum(output_terms.reshape(reps, share, width), axis=0)
    query_share, output_flip = lax.psum((query_local, output_local), "fs")
    output_share = output_flip.T
    query_moment_new = BETA * query_moment + (1.0 - BETA) * query_share
    output_moment_new = BETA * output_moment + (1.0 - BETA) * output_share
    query_squares, output_squares = lax.psum(
        (
            jnp.sum(query_moment_new * query_moment_new),
            jnp.sum(output_moment_new * output_moment_new),
        ),
        ("rep", "tp"),
    )
    entries = rank * query_moment.shape[1] * lax.axis_size("tp")
    query_dir = (query_moment_new * lax.rsqrt(query_squares / entries + EPS)).astype(jnp.bfloat16)
    output_dir = (output_moment_new * lax.rsqrt(output_squares / entries + EPS)).astype(
        jnp.bfloat16
    )
    query_full, output_full = (
        lax.all_gather(query_dir, "rep", axis=0, tiled=True),
        lax.all_gather(output_dir, "rep", axis=1, tiled=True),
    )
    query_step = jnp.dot(query_basis, query_full, preferred_element_type=jnp.float32)
    output_step = jnp.dot(output_full, output_basis.T, preferred_element_type=jnp.float32)
    query_new = query_weight - RATE * query_step
    output_new = output_weight - RATE * output_step
    return (
        query_step,
        output_step,
        query_new,
        output_new,
        query_new.astype(jnp.bfloat16),
        output_new.astype(jnp.bfloat16),
        query_moment_new,
        output_moment_new,
    )


MESH = pl.DeviceIdType.MESH
UNITS = 4


def exchange_kernel(
    si_hbm, oc_hbm, qc_hbm, ao_hbm, qb_hbm, ob_hbm, mq_hbm, mo_hbm,
    full, mom, total_sq,
    act, cot, head, base, old, mo, gath, own, pb, t1, sb, t2, ag, nrm, zb, zt, yb, yt,
    load_sem, sent, cx_r, az_r, aw_r, b1_r, b2_r, g_r, n_r, d_r, z_r,
):
    f, r, t = lax.axis_index("fs"), lax.axis_index("rep"), lax.axis_index("tp")
    y, x = r // 2, r % 2
    ot = 1 - t
    fpeer = [3 - f, (f + 2) % 4, f + 1 - 2 * (f % 2)]
    rpeer = [2 * y + (1 - x), 2 * (1 - y) + x, 3 - r]
    depth, half = base.shape[1], base.shape[2]
    hd = depth // 2
    qd = depth // 4
    share = half // 2
    cut = share // 2
    piece = cut // 4

    cols = pl.ds(pl.multiple_of(t * half, half), half)
    first = pl.ds(pl.multiple_of(r * qd, qd), qd)
    loads = []
    for k, (src, dst) in enumerate((
        (qb_hbm.at[first, cols], head), (qb_hbm.at[:, cols], base.at[0]), (ob_hbm.at[:, cols], base.at[1]),
        (qc_hbm, cot.at[0, t]), (ao_hbm, cot.at[1, t]),
        (si_hbm, act.at[0]), (oc_hbm, act.at[1]),
        (mq_hbm, old.at[0]), (mo_hbm, mo),
    )):
        c = pltpu.make_async_copy(src, dst, load_sem.at[k])
        c.start()
        loads.append(c)

    barrier = pltpu.get_barrier_semaphore()
    for g in fpeer:
        pl.semaphore_signal(barrier, inc=1, device_id=(g, r, t), device_id_type=MESH)
    for q in rpeer:
        for s in (t, ot):
            pl.semaphore_signal(barrier, inc=1, device_id=(f, q, s), device_id_type=MESH)
    pl.semaphore_signal(barrier, inc=1, device_id=(f, r, ot), device_id_type=MESH)

    def deal(p, rows, block):
        lo, hi = block[:, :share], block[:, share:]
        gath[p, f, rows, :share] = jnp.concatenate([lo[:, :cut], hi[:, :cut]], axis=1)
        gath[p, f, rows, share:] = jnp.concatenate([lo[:, cut:], hi[:, cut:]], axis=1)

    loads[0].wait()
    deal(0, first, head[...])
    pl.semaphore_wait(barrier, 10)

    def remote(src, dst, ss, rs, dev):
        return pltpu.make_async_remote_copy(
            src_ref=src, dst_ref=dst, send_sem=ss, recv_sem=rs, device_id=dev, device_id_type=MESH
        )

    def settle(ref, sem):
        pltpu.make_async_copy(ref, ref, sem).wait()

    h = x * (1 - t) + y * t
    near = rpeer[0] * (1 - t) + rpeer[1] * t
    mine = (
        first,
        pl.ds(pl.multiple_of(h * hd, hd), hd),
    )
    last = 3

    def unit_ref(u, slab):
        k = u % 2
        return gath.at[u // 2, slab, mine[u // 2], k * share : (k + 1) * share]

    def line(u, way, s, arrive=False):
        step = -1 if way == 0 else 1
        slab = f + step * s + (step if arrive else 0)
        ref = unit_ref(u, slab)
        dev = f + step if arrive else f - step
        to = f if arrive else dev
        slot = s if way == 0 else to + s
        return remote(ref, ref, sent.at[min(s, 1)], az_r.at[u, slot], (dev, r, t))

    def sends_line(way, s):
        return (f >= s) & (f < last) if way == 0 else (f + s <= last) & (f > 0)

    def gets_line(way, s):
        return f >= s + 1 if way == 0 else f + s + 1 <= last

    def carried(way):
        return f if way == 0 else last - f

    def share_slab(u, slab, slot):
        ref = unit_ref(u, slab)
        for q in (rpeer[2], rpeer[0], rpeer[1]) if u < 2 else (near,):
            remote(ref, ref, sent.at[2 if u < 2 else 9], aw_r.at[u, slot], (f, q, t)).start()

    def open_line(u, last_only=None):
        for way in range(2):
            go = sends_line(way, 0)
            if last_only is not None:
                go = go & ((carried(way) == 0) == last_only)

            @pl.when(go)
            def _():
                line(u, way, 0).start()

    def run_line(u, s):
        for way in range(2):
            @pl.when(gets_line(way, s))
            def _():
                line(u, way, s, True).wait_recv()
            if s < 2:
                @pl.when(sends_line(way, s + 1))
                def _():
                    line(u, way, s + 1).start()

            @pl.when(gets_line(way, s))
            def _():
                slab = f - 1 - s if way == 0 else f + 1 + s
                share_slab(u, slab, s if way == 0 else f + s)

    def swap_cot(p):
        ref = cot.at[p, t]
        return remote(ref, ref, sent.at[3], cx_r.at[p], (f, r, ot))

    def to_reps(u, k):
        j = 1 - x if k < 2 else x
        c = (0, 1, ot, t)[k]
        return remote(
            pb.at[u - 1, j, c], t1.at[u, r], sent.at[4], b1_r.at[u], (f, 2 * t + j, c)
        )

    def scatter_zs():
        for k in range(3):
            remote(
                zb.at[fpeer[k]], zt.at[k], sent.at[10], z_r.at[0], (fpeer[k], r, t)
            ).start()

    def to_owner(k):
        j = 1 - x if k < 2 else x
        c = (0, 1, ot, t)[k]
        return remote(yb.at[j, c], yt.at[r], sent.at[11], z_r.at[1], (f, 2 * t + j, c))

    def scatter_owners():
        settle(zt, z_r.at[0])
        total = zb[f].astype(jnp.float32)
        for k in range(3):
            total = total + zt[k].astype(jnp.float32)
        yb[...] = total.astype(jnp.bfloat16)
        for k in range(3):
            to_owner(k).start()

        @pl.when(t != y)
        def _():
            to_owner(3).start()

        @pl.when(t == y)
        def _():
            yt[r] = yb[x, t]

    def spread_own():
        @pl.when(t != y)
        def _():
            settle(yt, z_r.at[1])

        @pl.when(t == y)
        def _():
            settle(yt.at[:3], z_r.at[1])

        total = yt[0].astype(jnp.float32)
        for q in range(1, 4):
            total = total + yt[q].astype(jnp.float32)
        send_sums(0, total)

    def spread_sums():
        for k in (2, 1, 0):
            settle(ag.at[2, fpeer[k]], g_r.at[2, k])
            update_own(2, fpeer[k])

    def spread_zs():
        rows = rows_at(2, f)
        for j in range(3):
            ref = full.at[1, rpeer[j], rows, :]
            settle(ref, z_r.at[2 + j])
            for k in range(3):
                remote(ref, ref, sent.at[12], z_r.at[5], (fpeer[k], r, t)).start()

    def slab_dot(p, g, lanes):
        at = pl.ds(pl.multiple_of(g * depth, depth), depth)
        return jnp.dot(act[p, :, at], gath[p, g, :, lanes], preferred_element_type=jnp.float32)

    def lanes_of(us):
        return slice((us[0] % 2) * share, (us[-1] % 2 + 1) * share)

    def partial(p, us, slot):
        lanes = lanes_of(us)
        settle(gath.at[p, 0, : depth - (qd, hd)[p], lanes], aw_r.at[us[0], slot])
        slab = jnp.where(slot < f, f - 1 - slot, slot + 1)
        return own[p, :, lanes] + slab_dot(p, slab, lanes)

    def prepare(p, us, slot):
        own[p, :, lanes_of(us)] = partial(p, us, slot)

    def project(p, us):
        part = partial(p, us, 2)
        part = part.astype(jnp.bfloat16)
        for i, u in reversed(tuple(enumerate(us))):
            for c in range(2):
                terms = lax.dot_general(
                    part[:, i * share : (i + 1) * share], cot[p, c], (((0,), (0,)), ((), ())),
                    preferred_element_type=jnp.float32,
                )
                for j in range(2):
                    block = terms[j * cut : (j + 1) * cut].astype(jnp.bfloat16)
                    if u > 0:
                        pb[u - 1, j, c] = block
                    else:
                        for g in range(4):
                            zb[g, j, c] = block[g * piece : (g + 1) * piece]
            if u > 0:
                scatter_reps(u)
            else:
                scatter_zs()

    def scatter_reps(u):
        for k in range(3):
            to_reps(u, k).start()

        @pl.when(t != y)
        def _():
            to_reps(u, 3).start()

        @pl.when(t == y)
        def _():
            t1[u, r] = pb[u - 1, x, t]

    def scatter_tokens(u):
        @pl.when(t != y)
        def _():
            settle(t1.at[u], b1_r.at[u])

        @pl.when(t == y)
        def _():
            settle(t1.at[u, :3], b1_r.at[u])

        total = t1[u, 0].astype(jnp.float32)
        for q in range(1, 4):
            total = total + t1[u, q].astype(jnp.float32)
        for g in range(4):
            sb[u, g] = total[g * piece : (g + 1) * piece].astype(jnp.bfloat16)
        for k in range(3):
            to_token(u, k).start()

    def to_token(u, k):
        return remote(
            sb.at[u, fpeer[k]], t2.at[u, k], sent.at[5], b2_r.at[u], (fpeer[k], r, t)
        )

    def rows_at(u, g):
        at = (u % 2) * cut + g * piece
        return pl.ds(pl.multiple_of(at, piece), piece)

    def to_dirs(u, g, k):
        ref = full.at[u // 2, r, rows_at(u, g), :]
        ss, rs = (sent.at[12], z_r.at[2 + k]) if u == 2 else (sent.at[7], d_r.at[u // 2])
        return remote(ref, ref, ss, rs, (f, rpeer[k], t))

    def to_sums(u, k):
        return remote(
            ag.at[u, f], ag.at[u, f], sent.at[6], g_r.at[u, k], (fpeer[k], r, t)
        )

    def update_own(u, g):
        p, rows = u // 2, rows_at(u, g)
        new = BETA * old[p, rows, :] + (1.0 - BETA) * ag[u, g].astype(jnp.float32)
        mom[p, rows, :] = new
        full[p, r, rows, :] = new.astype(jnp.bfloat16)

    def update(u, g):
        update_own(u, g)
        for k in (2, 0, 1):
            to_dirs(u, g, k).start()

    def send_sums(u, total):
        ag[u, f] = total.astype(jnp.bfloat16)
        for k in range(3):
            to_sums(u, k).start()
        update(u, f)

    def gather_sums(u):
        total = sb[u, f].astype(jnp.float32)
        settle(t2.at[u], b2_r.at[u])
        for k in range(3):
            total = total + t2[u, k].astype(jnp.float32)
        send_sums(u, total)

    def gather_dirs(u):
        for k in (2, 1, 0):
            settle(ag.at[u, fpeer[k]], g_r.at[u, k])
            update(u, fpeer[k])

    others = [(q, s) for q in rpeer for s in (t, ot)] + [(r, ot)]
    me = 2 * r + t

    def to_norms(p, k):
        q, s = others[k]
        ref = nrm.at[p, me]
        return remote(ref, ref, sent.at[8], n_r.at[p], (f, q, s))

    def send_norms(p):
        sq = mom[p] * mom[p]
        lanes = sq[:, :128]
        for k in range(1, sq.shape[1] // 128):
            lanes = lanes + sq[:, k * 128 : (k + 1) * 128]
        acc = lanes[:8]
        for k in range(1, share // 8):
            acc = acc + lanes[k * 8 : (k + 1) * 8]
        nrm[p, me] = acc
        for k in range(7):
            to_norms(p, k).start()

    def sum_norms(p):
        settle(nrm.at[p, :7], n_r.at[p])
        acc = nrm[p, 0]
        for k in range(1, 8):
            acc = acc + nrm[p, k]
        total_sq[p] = acc

    def finish(p):
        sum_norms(p)
        if p == 0:
            settle(full.at[0, :3], d_r.at[0])
        else:
            settle(full.at[1, :3, : 3 * piece, :], z_r.at[5])
            settle(full.at[1, :3, :cut, :], d_r.at[1])

    open_line(1)
    open_line(0)
    loads[2].wait()
    deal(1, slice(None), base[1])
    open_line(2)
    open_line(3, True)
    loads[1].wait()
    for k in range(1, 4):
        rows = pl.ds(pl.multiple_of((r + k) % 4 * qd, qd), qd)
        deal(0, rows, base[0, rows, :])
    for p in range(2):
        loads[3 + p].wait()
        swap_cot(p).start()
    loads[7].wait()
    loads[8].wait()
    old[1] = mo[...].T
    for p in range(2):
        loads[5 + p].wait()
        own[p] = slab_dot(p, f, slice(None))
        settle(cot.at[p, ot], cx_r.at[p])
    run_line(1, 0)
    run_line(0, 0)
    open_line(3, False)
    run_line(1, 1)
    run_line(0, 1)
    run_line(2, 0)
    run_line(1, 2)
    run_line(0, 2)
    run_line(3, 0)
    run_line(2, 1)
    run_line(3, 1)
    prepare(0, (1,), 0)
    prepare(0, (0,), 0)
    prepare(0, (1,), 1)
    run_line(2, 2)
    project(0, (1,))
    run_line(3, 2)
    prepare(0, (0,), 1)
    project(0, (0,))
    prepare(1, (2,), 0)
    prepare(1, (2,), 1)
    project(1, (2,))
    prepare(1, (3,), 0)
    prepare(1, (3,), 1)
    project(1, (3,))
    scatter_tokens(1)
    scatter_owners()
    scatter_tokens(2)
    gather_sums(1)
    scatter_tokens(3)
    spread_own()
    gather_sums(2)
    gather_dirs(1)
    gather_sums(3)
    gather_dirs(0)
    send_norms(0)
    spread_zs()
    spread_sums()
    gather_dirs(3)
    send_norms(1)
    finish(0)
    finish(1)
    inner = (f > 0) & (f < last)

    @pl.when(inner)
    def _():
        settle(gath.at[0, :3, :, :share], sent.at[0])
        settle(gath.at[0, :3, : depth - qd], sent.at[1])

    @pl.when(jnp.logical_not(inner))
    def _():
        settle(gath.at[0, :3, :hd, :share], sent.at[0])

    for k in range(2):
        settle(gath.at[k, :3, : depth - (qd, hd)[k], :], sent.at[2 + 7 * k])
    settle(cot.at[0], sent.at[3])

    @pl.when(t != y)
    def _():
        settle(pb, sent.at[4])
        settle(yt, sent.at[11])

    @pl.when(t == y)
    def _():
        settle(pb.at[:, :, :, : 3 * piece], sent.at[4])
        settle(yt.at[:3], sent.at[11])

    settle(t2.at[:3], sent.at[5])
    settle(t2, sent.at[6])
    settle(full.at[:, :3, : 6 * piece], sent.at[7])
    settle(nrm.at[:, :7], sent.at[8])
    settle(zt, sent.at[10])
    settle(t2, sent.at[12])


def finish_kernel(
    entries, qb, ob, fq, fo, sq, qw, ow, mq, mo,
    qs_o, os_o, qn_o, on_o, qc_o, oc_o, mq_o, mo_o,
):
    def scale(p):
        rows = jnp.sum(sq[p], axis=0, keepdims=True)
        return lax.rsqrt(jnp.sum(rows, axis=1, keepdims=True) / entries + EPS)

    step = jnp.dot(qb[...], fq[0], preferred_element_type=jnp.float32) * scale(0)
    new = qw[...] - RATE * step
    qs_o[...] = step
    qn_o[...] = new
    qc_o[...] = new.astype(jnp.bfloat16)
    step = lax.dot_general(
        fo[0].T, ob[...], (((1,), (1,)), ((), ())), preferred_element_type=jnp.float32
    ) * scale(1)
    new = ow[...] - RATE * step
    os_o[...] = step
    on_o[...] = new
    oc_o[...] = new.astype(jnp.bfloat16)
    mq_o[...] = mq[0]
    mo_o[...] = mo[0].T


def on_device_fast(
    saved_input, query_cot, attn_out, out_cot, query_basis, output_basis,
    query_weight, output_weight, query_moment, output_moment,
):
    tokens, depth_all = saved_input.shape
    width = query_cot.shape[1]
    depth, rank = query_basis.shape
    share = rank // 4
    cut = share // 2
    piece = cut // 4
    entries = rank * width * lax.axis_size("tp")
    bf, f32 = jnp.bfloat16, jnp.float32
    any_spec = pl.BlockSpec(memory_space=pl.ANY)
    dma = pltpu.SemaphoreType.DMA
    ins = (
        saved_input, out_cot, query_cot, attn_out, query_basis, output_basis,
        query_moment, output_moment,
    )
    full, mom, norm = pl.pallas_call(
        exchange_kernel,
        out_shape=(
            jax.ShapeDtypeStruct((2, 4, share, width), bf),
            jax.ShapeDtypeStruct((2, share, width), f32),
            jax.ShapeDtypeStruct((2, 8, 128), f32),
        ),
        in_specs=[any_spec] * 8,
        out_specs=(pl.BlockSpec(memory_space=pltpu.VMEM),) * 3,
        scratch_shapes=[
            pltpu.VMEM((2, tokens, depth_all), bf),
            pltpu.VMEM((2, 2, tokens, width), bf),
            pltpu.VMEM((depth // 4, rank // 2), bf),
            pltpu.VMEM((2, depth, rank // 2), bf),
            pltpu.VMEM((2, share, width), f32),
            pltpu.VMEM((width, share), f32),
            pltpu.VMEM((2, 4, depth, 2 * share), bf),
            pltpu.VMEM((2, tokens, 2 * share), f32),
            pltpu.VMEM((UNITS - 1, 2, 2, cut, width), bf),
            pltpu.VMEM((UNITS, 4, cut, width), bf),
            pltpu.VMEM((UNITS, 4, piece, width), bf),
            pltpu.VMEM((UNITS, 3, piece, width), bf),
            pltpu.VMEM((UNITS, 4, piece, width), bf),
            pltpu.VMEM((2, 8, 8, 128), f32),
            pltpu.VMEM((4, 2, 2, piece, width), bf),
            pltpu.VMEM((3, 2, 2, piece, width), bf),
            pltpu.VMEM((2, 2, piece, width), bf),
            pltpu.VMEM((4, piece, width), bf),
            dma((9,)), dma((13,)), dma((2,)), dma((UNITS, 3)), dma((UNITS, 3)), dma((UNITS,)),
            dma((UNITS,)), dma((UNITS, 3)), dma((2,)), dma((2,)), dma((6,)),
        ],
        compiler_params=pltpu.CompilerParams(
            collective_id=0, has_side_effects=True, vmem_limit_bytes=20 * 2**20
        ),
    )(*(pltpu.with_memory_space_constraint(a, pltpu.HBM) for a in ins))
    full = full.reshape(2, rank, width)
    n = 2
    rows = pl.BlockSpec((depth // n, rank), lambda i: (i, 0))
    whole = pl.BlockSpec((depth, rank), lambda i: (0, 0))
    wq = pl.BlockSpec((depth // n, width), lambda i: (i, 0))
    wo = pl.BlockSpec((width // n, depth), lambda i: (i, 0))
    mq = pl.BlockSpec((share // n, width), lambda i: (i, 0))
    mo = pl.BlockSpec((width // n, share), lambda i: (i, 0))
    sq, so = query_weight.shape, output_weight.shape
    return pl.pallas_call(
        functools.partial(finish_kernel, entries),
        grid=(n,),
        out_shape=tuple(
            jax.ShapeDtypeStruct(s, d)
            for s, d in (
                (sq, f32), (so, f32), (sq, f32), (so, f32), (sq, bf), (so, bf),
                (query_moment.shape, f32), (output_moment.shape, f32),
            )
        ),
        in_specs=[
            rows, whole,
            pl.BlockSpec((1, rank, width), lambda i: (0, 0, 0)),
            pl.BlockSpec((1, rank, width // n), lambda i: (1, 0, i)),
            pl.BlockSpec((2, 8, 128), lambda i: (0, 0, 0)),
            wq, wo,
            pl.BlockSpec((1, share // n, width), lambda i: (0, i, 0)),
            pl.BlockSpec((1, share, width // n), lambda i: (1, 0, i)),
        ],
        out_specs=(wq, wo, wq, wo, wq, wo, mq, mo),
        cost_estimate=pl.CostEstimate(
            flops=4 * depth * rank * width, bytes_accessed=20 * depth * width, transcendentals=0
        ),
        compiler_params=pltpu.CompilerParams(vmem_limit_bytes=20 * 2**20),
    )(query_basis, output_basis, full, full, norm, query_weight, output_weight, mom, mom)


def solution(mesh):
    small = dict(mesh.shape) == {"fs": 4, "rep": 4, "tp": 2}
    body = on_device_fast if small else on_device
    placed = (
        P(("fs", "rep"), None),
        P(("fs", "rep"), "tp"),
        P(("fs", "rep"), "tp"),
        P(("fs", "rep"), None),
        P("fs", None),
        P("fs", None),
        P("fs", "tp"),
        P("tp", "fs"),
        P("rep", "tp"),
        P("tp", "rep"),
    )
    return jax.shard_map(
        body,
        mesh=mesh,
        in_specs=placed,
        out_specs=(
            P("fs", "tp"),
            P("tp", "fs"),
            P("fs", "tp"),
            P("tp", "fs"),
            P("fs", "tp"),
            P("tp", "fs"),
            P("rep", "tp"),
            P("tp", "rep"),
        ),
        check_vma=False,
    )
```

```python
import functools

import jax
import jax.numpy as jnp
from jax import lax
from jax.experimental import pallas as pl
from jax.experimental.pallas import tpu as pltpu
from jax.sharding import PartitionSpec as P

BETA = 0.8
RATE = 0.2
EPS = 1e-06


def on_device(
    saved_input,
    query_cot,
    attn_out,
    out_cot,
    query_basis,
    output_basis,
    query_weight,
    output_weight,
    query_moment,
    output_moment,
):
    rank = query_basis.shape[1]
    grad_rows = lax.psum_scatter(
        jnp.dot(saved_input.T, query_cot, preferred_element_type=jnp.float32),
        "fs",
        scatter_dimension=0,
        tiled=True,
    )
    query_part = jnp.dot(
        query_basis.astype(jnp.float32).T, grad_rows, precision=lax.Precision.HIGHEST
    )
    cot_proj = jnp.dot(
        out_cot,
        lax.all_gather(output_basis, "fs", axis=0, tiled=True),
        preferred_element_type=jnp.float32,
    )
    output_part = jnp.dot(attn_out.astype(jnp.float32).T, cot_proj, precision=lax.Precision.HIGHEST)
    reps = lax.axis_size("rep")
    share = rank // reps
    query_terms, output_terms = (
        lax.all_to_all(
            query_part.astype(jnp.bfloat16), "rep", split_axis=0, concat_axis=0, tiled=True
        ).astype(query_part.dtype),
        lax.all_to_all(
            output_part.T.astype(jnp.bfloat16), "rep", split_axis=0, concat_axis=0, tiled=True
        ).astype(jnp.float32),
    )
    width = query_part.shape[1]
    query_local = jnp.sum(query_terms.reshape(reps, share, width), axis=0)
    output_local = jnp.sum(output_terms.reshape(reps, share, width), axis=0)
    query_share, output_flip = lax.psum((query_local, output_local), "fs")
    output_share = output_flip.T
    query_moment_new = BETA * query_moment + (1.0 - BETA) * query_share
    output_moment_new = BETA * output_moment + (1.0 - BETA) * output_share
    query_squares, output_squares = lax.psum(
        (
            jnp.sum(query_moment_new * query_moment_new),
            jnp.sum(output_moment_new * output_moment_new),
        ),
        ("rep", "tp"),
    )
    entries = rank * query_moment.shape[1] * lax.axis_size("tp")
    query_dir = (query_moment_new * lax.rsqrt(query_squares / entries + EPS)).astype(jnp.bfloat16)
    output_dir = (output_moment_new * lax.rsqrt(output_squares / entries + EPS)).astype(
        jnp.bfloat16
    )
    query_full, output_full = (
        lax.all_gather(query_dir, "rep", axis=0, tiled=True),
        lax.all_gather(output_dir, "rep", axis=1, tiled=True),
    )
    query_step = jnp.dot(query_basis, query_full, preferred_element_type=jnp.float32)
    output_step = jnp.dot(output_full, output_basis.T, preferred_element_type=jnp.float32)
    query_new = query_weight - RATE * query_step
    output_new = output_weight - RATE * output_step
    return (
        query_step,
        output_step,
        query_new,
        output_new,
        query_new.astype(jnp.bfloat16),
        output_new.astype(jnp.bfloat16),
        query_moment_new,
        output_moment_new,
    )


MESH = pl.DeviceIdType.MESH
UNITS = 4


def exchange_kernel(
    si_hbm, oc_hbm, qc_hbm, ao_hbm, qb_hbm, ob_hbm, mq_hbm, mo_hbm,
    full, mom, total_sq,
    act, cot, head, base, old, mo, gath, own, pb, t1, sb, t2, ag, nrm, zb, zt, yb, yt,
    load_sem, sent, cx_r, az_r, aw_r, b1_r, b2_r, g_r, n_r, d_r, z_r,
):
    f, r, t = lax.axis_index("fs"), lax.axis_index("rep"), lax.axis_index("tp")
    y, x = r // 2, r % 2
    ot = 1 - t
    fpeer = [3 - f, (f + 2) % 4, f + 1 - 2 * (f % 2)]
    rpeer = [2 * y + (1 - x), 2 * (1 - y) + x, 3 - r]
    depth, half = base.shape[1], base.shape[2]
    hd = depth // 2
    qd = depth // 4
    share = half // 2
    cut = share // 2
    piece = cut // 4

    cols = pl.ds(pl.multiple_of(t * half, half), half)
    first = pl.ds(pl.multiple_of(r * qd, qd), qd)
    loads = []
    for k, (src, dst) in enumerate((
        (qb_hbm.at[first, cols], head), (qb_hbm.at[:, cols], base.at[0]), (ob_hbm.at[:, cols], base.at[1]),
        (qc_hbm, cot.at[0, t]), (ao_hbm, cot.at[1, t]),
        (si_hbm, act.at[0]), (oc_hbm, act.at[1]),
        (mq_hbm, old.at[0]), (mo_hbm, mo),
    )):
        c = pltpu.make_async_copy(src, dst, load_sem.at[k])
        c.start()
        loads.append(c)

    barrier = pltpu.get_barrier_semaphore()
    for g in fpeer:
        pl.semaphore_signal(barrier, inc=1, device_id=(g, r, t), device_id_type=MESH)
    for q in rpeer:
        for s in (t, ot):
            pl.semaphore_signal(barrier, inc=1, device_id=(f, q, s), device_id_type=MESH)
    pl.semaphore_signal(barrier, inc=1, device_id=(f, r, ot), device_id_type=MESH)

    def deal(p, rows, block):
        lo, hi = block[:, :share], block[:, share:]
        gath[p, f, rows, :share] = jnp.concatenate([lo[:, :cut], hi[:, :cut]], axis=1)
        gath[p, f, rows, share:] = jnp.concatenate([lo[:, cut:], hi[:, cut:]], axis=1)

    loads[0].wait()
    deal(0, first, head[...])
    pl.semaphore_wait(barrier, 10)

    def remote(src, dst, ss, rs, dev):
        return pltpu.make_async_remote_copy(
            src_ref=src, dst_ref=dst, send_sem=ss, recv_sem=rs, device_id=dev, device_id_type=MESH
        )

    def settle(ref, sem):
        pltpu.make_async_copy(ref, ref, sem).wait()

    h = x * (1 - t) + y * t
    near = rpeer[0] * (1 - t) + rpeer[1] * t
    mine = (
        first,
        pl.ds(pl.multiple_of(h * hd, hd), hd),
    )
    last = 3

    def unit_ref(u, slab):
        k = u % 2
        return gath.at[u // 2, slab, mine[u // 2], k * share : (k + 1) * share]

    def line(u, way, s, arrive=False):
        step = -1 if way == 0 else 1
        slab = f + step * s + (step if arrive else 0)
        ref = unit_ref(u, slab)
        dev = f + step if arrive else f - step
        to = f if arrive else dev
        slot = s if way == 0 else to + s
        return remote(ref, ref, sent.at[min(s, 1)], az_r.at[u, slot], (dev, r, t))

    def sends_line(way, s):
        return (f >= s) & (f < last) if way == 0 else (f + s <= last) & (f > 0)

    def gets_line(way, s):
        return f >= s + 1 if way == 0 else f + s + 1 <= last

    def carried(way):
        return f if way == 0 else last - f

    def share_slab(u, slab, slot):
        ref = unit_ref(u, slab)
        for q in (rpeer[2], rpeer[0], rpeer[1]) if u < 2 else (near,):
            remote(ref, ref, sent.at[2 if u < 2 else 9], aw_r.at[u, slot], (f, q, t)).start()

    def open_line(u, last_only=None):
        for way in range(2):
            go = sends_line(way, 0)
            if last_only is not None:
                go = go & ((carried(way) == 0) == last_only)

            @pl.when(go)
            def _():
                line(u, way, 0).start()

    def run_line(u, s):
        for way in range(2):
            @pl.when(gets_line(way, s))
            def _():
                line(u, way, s, True).wait_recv()
            if s < 2:
                @pl.when(sends_line(way, s + 1))
                def _():
                    line(u, way, s + 1).start()

            @pl.when(gets_line(way, s))
            def _():
                slab = f - 1 - s if way == 0 else f + 1 + s
                share_slab(u, slab, s if way == 0 else f + s)

    def swap_cot(p):
        ref = cot.at[p, t]
        return remote(ref, ref, sent.at[3], cx_r.at[p], (f, r, ot))

    def to_reps(u, k):
        j = 1 - x if k < 2 else x
        c = (0, 1, ot, t)[k]
        return remote(
            pb.at[u - 1, j, c], t1.at[u, r], sent.at[4], b1_r.at[u], (f, 2 * t + j, c)
        )

    def scatter_zs():
        for k in range(3):
            remote(
                zb.at[fpeer[k]], zt.at[k], sent.at[10], z_r.at[0], (fpeer[k], r, t)
            ).start()

    def to_owner(k):
        j = 1 - x if k < 2 else x
        c = (0, 1, ot, t)[k]
        return remote(yb.at[j, c], yt.at[r], sent.at[11], z_r.at[1], (f, 2 * t + j, c))

    def scatter_owners():
        settle(zt, z_r.at[0])
        total = zb[f].astype(jnp.float32)
        for k in range(3):
            total = total + zt[k].astype(jnp.float32)
        yb[...] = total.astype(jnp.bfloat16)
        for k in range(3):
            to_owner(k).start()

        @pl.when(t != y)
        def _():
            to_owner(3).start()

        @pl.when(t == y)
        def _():
            yt[r] = yb[x, t]

    def spread_own():
        @pl.when(t != y)
        def _():
            settle(yt, z_r.at[1])

        @pl.when(t == y)
        def _():
            settle(yt.at[:3], z_r.at[1])

        total = yt[0].astype(jnp.float32)
        for q in range(1, 4):
            total = total + yt[q].astype(jnp.float32)
        send_sums(0, total)

    def spread_sums():
        for k in (2, 1, 0):
            settle(ag.at[2, fpeer[k]], g_r.at[2, k])
            update_own(2, fpeer[k])

    def spread_zs():
        rows = rows_at(2, f)
        for j in range(3):
            ref = full.at[1, rpeer[j], rows, :]
            settle(ref, z_r.at[2 + j])
            for k in range(3):
                remote(ref, ref, sent.at[12], z_r.at[5], (fpeer[k], r, t)).start()

    def slab_dot(p, g, lanes):
        at = pl.ds(pl.multiple_of(g * depth, depth), depth)
        return jnp.dot(act[p, :, at], gath[p, g, :, lanes], preferred_element_type=jnp.float32)

    def lanes_of(us):
        return slice((us[0] % 2) * share, (us[-1] % 2 + 1) * share)

    def partial(p, us, slot):
        lanes = lanes_of(us)
        settle(gath.at[p, 0, : depth - (qd, hd)[p], lanes], aw_r.at[us[0], slot])
        slab = jnp.where(slot < f, f - 1 - slot, slot + 1)
        return own[p, :, lanes] + slab_dot(p, slab, lanes)

    def prepare(p, us, slot):
        own[p, :, lanes_of(us)] = partial(p, us, slot)

    def project(p, us):
        part = partial(p, us, 2)
        part = part.astype(jnp.bfloat16)
        for i, u in reversed(tuple(enumerate(us))):
            for c in range(2):
                terms = lax.dot_general(
                    part[:, i * share : (i + 1) * share], cot[p, c], (((0,), (0,)), ((), ())),
                    preferred_element_type=jnp.float32,
                )
                for j in range(2):
                    block = terms[j * cut : (j + 1) * cut].astype(jnp.bfloat16)
                    if u > 0:
                        pb[u - 1, j, c] = block
                    else:
                        for g in range(4):
                            zb[g, j, c] = block[g * piece : (g + 1) * piece]
            if u > 0:
                scatter_reps(u)
            else:
                scatter_zs()

    def scatter_reps(u):
        for k in range(3):
            to_reps(u, k).start()

        @pl.when(t != y)
        def _():
            to_reps(u, 3).start()

        @pl.when(t == y)
        def _():
            t1[u, r] = pb[u - 1, x, t]

    def scatter_tokens(u):
        @pl.when(t != y)
        def _():
            settle(t1.at[u], b1_r.at[u])

        @pl.when(t == y)
        def _():
            settle(t1.at[u, :3], b1_r.at[u])

        total = t1[u, 0].astype(jnp.float32)
        for q in range(1, 4):
            total = total + t1[u, q].astype(jnp.float32)
        for g in range(4):
            sb[u, g] = total[g * piece : (g + 1) * piece].astype(jnp.bfloat16)
        for k in range(3):
            to_token(u, k).start()

    def to_token(u, k):
        return remote(
            sb.at[u, fpeer[k]], t2.at[u, k], sent.at[5], b2_r.at[u], (fpeer[k], r, t)
        )

    def rows_at(u, g):
        at = (u % 2) * cut + g * piece
        return pl.ds(pl.multiple_of(at, piece), piece)

    def to_dirs(u, g, k):
        ref = full.at[u // 2, r, rows_at(u, g), :]
        ss, rs = (sent.at[12], z_r.at[2 + k]) if u == 2 else (sent.at[7], d_r.at[u // 2])
        return remote(ref, ref, ss, rs, (f, rpeer[k], t))

    def to_sums(u, k):
        return remote(
            ag.at[u, f], ag.at[u, f], sent.at[6], g_r.at[u, k], (fpeer[k], r, t)
        )

    def update_own(u, g):
        p, rows = u // 2, rows_at(u, g)
        new = BETA * old[p, rows, :] + (1.0 - BETA) * ag[u, g].astype(jnp.float32)
        mom[p, rows, :] = new
        full[p, r, rows, :] = new.astype(jnp.bfloat16)

    def update(u, g):
        update_own(u, g)
        for k in (2, 0, 1):
            to_dirs(u, g, k).start()

    def send_sums(u, total):
        ag[u, f] = total.astype(jnp.bfloat16)
        for k in range(3):
            to_sums(u, k).start()
        update(u, f)

    def gather_sums(u):
        total = sb[u, f].astype(jnp.float32)
        settle(t2.at[u], b2_r.at[u])
        for k in range(3):
            total = total + t2[u, k].astype(jnp.float32)
        send_sums(u, total)

    def gather_dirs(u):
        for k in (2, 1, 0):
            settle(ag.at[u, fpeer[k]], g_r.at[u, k])
            update(u, fpeer[k])

    others = [(q, s) for q in rpeer for s in (t, ot)] + [(r, ot)]
    me = 2 * r + t

    def to_norms(p, k):
        q, s = others[k]
        ref = nrm.at[p, me]
        return remote(ref, ref, sent.at[8], n_r.at[p], (f, q, s))

    def send_norms(p):
        sq = mom[p] * mom[p]
        lanes = sq[:, :128]
        for k in range(1, sq.shape[1] // 128):
            lanes = lanes + sq[:, k * 128 : (k + 1) * 128]
        acc = lanes[:8]
        for k in range(1, share // 8):
            acc = acc + lanes[k * 8 : (k + 1) * 8]
        nrm[p, me] = acc
        for k in range(7):
            to_norms(p, k).start()

    def sum_norms(p):
        settle(nrm.at[p, :7], n_r.at[p])
        acc = nrm[p, 0]
        for k in range(1, 8):
            acc = acc + nrm[p, k]
        total_sq[p] = acc

    def finish(p):
        sum_norms(p)
        if p == 0:
            settle(full.at[0, :3], d_r.at[0])
        else:
            settle(full.at[1, :3, : 3 * piece, :], z_r.at[5])
            settle(full.at[1, :3, :cut, :], d_r.at[1])

    open_line(1)
    open_line(0)
    loads[2].wait()
    deal(1, slice(None), base[1])
    open_line(2)
    open_line(3, True)
    loads[1].wait()
    for k in range(1, 4):
        rows = pl.ds(pl.multiple_of((r + k) % 4 * qd, qd), qd)
        deal(0, rows, base[0, rows, :])
    for p in range(2):
        loads[3 + p].wait()
        swap_cot(p).start()
    loads[7].wait()
    loads[8].wait()
    old[1] = mo[...].T
    for p in range(2):
        loads[5 + p].wait()
        own[p] = slab_dot(p, f, slice(None))
        settle(cot.at[p, ot], cx_r.at[p])
    run_line(1, 0)
    run_line(0, 0)
    open_line(3, False)
    run_line(1, 1)
    run_line(0, 1)
    run_line(2, 0)
    run_line(1, 2)
    run_line(0, 2)
    run_line(3, 0)
    run_line(2, 1)
    run_line(3, 1)
    prepare(0, (1,), 0)
    prepare(0, (0,), 0)
    prepare(0, (1,), 1)
    run_line(2, 2)
    prepare(0, (0,), 1)
    project(0, (1,))
    run_line(3, 2)
    project(0, (0,))
    prepare(1, (2,), 0)
    prepare(1, (2,), 1)
    project(1, (2,))
    prepare(1, (3,), 0)
    prepare(1, (3,), 1)
    project(1, (3,))
    scatter_tokens(1)
    scatter_owners()
    scatter_tokens(2)
    gather_sums(1)
    scatter_tokens(3)
    spread_own()
    gather_sums(2)
    gather_dirs(1)
    gather_sums(3)
    gather_dirs(0)
    send_norms(0)
    spread_zs()
    gather_dirs(3)
    spread_sums()
    send_norms(1)
    finish(0)
    finish(1)
    inner = (f > 0) & (f < last)

    @pl.when(inner)
    def _():
        settle(gath.at[0, :3, :, :share], sent.at[0])
        settle(gath.at[0, :3, : depth - qd], sent.at[1])

    @pl.when(jnp.logical_not(inner))
    def _():
        settle(gath.at[0, :3, :hd, :share], sent.at[0])

    for k in range(2):
        settle(gath.at[k, :3, : depth - (qd, hd)[k], :], sent.at[2 + 7 * k])
    settle(cot.at[0], sent.at[3])

    @pl.when(t != y)
    def _():
        settle(pb, sent.at[4])
        settle(yt, sent.at[11])

    @pl.when(t == y)
    def _():
        settle(pb.at[:, :, :, : 3 * piece], sent.at[4])
        settle(yt.at[:3], sent.at[11])

    settle(t2.at[:3], sent.at[5])
    settle(t2, sent.at[6])
    settle(full.at[:, :3, : 6 * piece], sent.at[7])
    settle(nrm.at[:, :7], sent.at[8])
    settle(zt, sent.at[10])
    settle(t2, sent.at[12])


def finish_kernel(
    entries, qb, ob, fq, fo, sq, qw, ow, mq, mo,
    qs_o, os_o, qn_o, on_o, qc_o, oc_o, mq_o, mo_o,
):
    def scale(p):
        rows = jnp.sum(sq[p], axis=0, keepdims=True)
        return lax.rsqrt(jnp.sum(rows, axis=1, keepdims=True) / entries + EPS)

    step = jnp.dot(qb[...], fq[0], preferred_element_type=jnp.float32) * scale(0)
    new = qw[...] - RATE * step
    qs_o[...] = step
    qn_o[...] = new
    qc_o[...] = new.astype(jnp.bfloat16)
    step = lax.dot_general(
        fo[0].T, ob[...], (((1,), (1,)), ((), ())), preferred_element_type=jnp.float32
    ) * scale(1)
    new = ow[...] - RATE * step
    os_o[...] = step
    on_o[...] = new
    oc_o[...] = new.astype(jnp.bfloat16)
    mq_o[...] = mq[0]
    mo_o[...] = mo[0].T


def on_device_fast(
    saved_input, query_cot, attn_out, out_cot, query_basis, output_basis,
    query_weight, output_weight, query_moment, output_moment,
):
    tokens, depth_all = saved_input.shape
    width = query_cot.shape[1]
    depth, rank = query_basis.shape
    share = rank // 4
    cut = share // 2
    piece = cut // 4
    entries = rank * width * lax.axis_size("tp")
    bf, f32 = jnp.bfloat16, jnp.float32
    any_spec = pl.BlockSpec(memory_space=pl.ANY)
    dma = pltpu.SemaphoreType.DMA
    ins = (
        saved_input, out_cot, query_cot, attn_out, query_basis, output_basis,
        query_moment, output_moment,
    )
    full, mom, norm = pl.pallas_call(
        exchange_kernel,
        out_shape=(
            jax.ShapeDtypeStruct((2, 4, share, width), bf),
            jax.ShapeDtypeStruct((2, share, width), f32),
            jax.ShapeDtypeStruct((2, 8, 128), f32),
        ),
        in_specs=[any_spec] * 8,
        out_specs=(pl.BlockSpec(memory_space=pltpu.VMEM),) * 3,
        scratch_shapes=[
            pltpu.VMEM((2, tokens, depth_all), bf),
            pltpu.VMEM((2, 2, tokens, width), bf),
            pltpu.VMEM((depth // 4, rank // 2), bf),
            pltpu.VMEM((2, depth, rank // 2), bf),
            pltpu.VMEM((2, share, width), f32),
            pltpu.VMEM((width, share), f32),
            pltpu.VMEM((2, 4, depth, 2 * share), bf),
            pltpu.VMEM((2, tokens, 2 * share), f32),
            pltpu.VMEM((UNITS - 1, 2, 2, cut, width), bf),
            pltpu.VMEM((UNITS, 4, cut, width), bf),
            pltpu.VMEM((UNITS, 4, piece, width), bf),
            pltpu.VMEM((UNITS, 3, piece, width), bf),
            pltpu.VMEM((UNITS, 4, piece, width), bf),
            pltpu.VMEM((2, 8, 8, 128), f32),
            pltpu.VMEM((4, 2, 2, piece, width), bf),
            pltpu.VMEM((3, 2, 2, piece, width), bf),
            pltpu.VMEM((2, 2, piece, width), bf),
            pltpu.VMEM((4, piece, width), bf),
            dma((9,)), dma((13,)), dma((2,)), dma((UNITS, 3)), dma((UNITS, 3)), dma((UNITS,)),
            dma((UNITS,)), dma((UNITS, 3)), dma((2,)), dma((2,)), dma((6,)),
        ],
        compiler_params=pltpu.CompilerParams(
            collective_id=0, has_side_effects=True, vmem_limit_bytes=20 * 2**20
        ),
    )(*(pltpu.with_memory_space_constraint(a, pltpu.HBM) for a in ins))
    full = full.reshape(2, rank, width)
    n = 2
    rows = pl.BlockSpec((depth // n, rank), lambda i: (i, 0))
    whole = pl.BlockSpec((depth, rank), lambda i: (0, 0))
    wq = pl.BlockSpec((depth // n, width), lambda i: (i, 0))
    wo = pl.BlockSpec((width // n, depth), lambda i: (i, 0))
    mq = pl.BlockSpec((share // n, width), lambda i: (i, 0))
    mo = pl.BlockSpec((width // n, share), lambda i: (i, 0))
    sq, so = query_weight.shape, output_weight.shape
    return pl.pallas_call(
        functools.partial(finish_kernel, entries),
        grid=(n,),
        out_shape=tuple(
            jax.ShapeDtypeStruct(s, d)
            for s, d in (
                (sq, f32), (so, f32), (sq, f32), (so, f32), (sq, bf), (so, bf),
                (query_moment.shape, f32), (output_moment.shape, f32),
            )
        ),
        in_specs=[
            rows, whole,
            pl.BlockSpec((1, rank, width), lambda i: (0, 0, 0)),
            pl.BlockSpec((1, rank, width // n), lambda i: (1, 0, i)),
            pl.BlockSpec((2, 8, 128), lambda i: (0, 0, 0)),
            wq, wo,
            pl.BlockSpec((1, share // n, width), lambda i: (0, i, 0)),
            pl.BlockSpec((1, share, width // n), lambda i: (1, 0, i)),
        ],
        out_specs=(wq, wo, wq, wo, wq, wo, mq, mo),
        cost_estimate=pl.CostEstimate(
            flops=4 * depth * rank * width, bytes_accessed=20 * depth * width, transcendentals=0
        ),
        compiler_params=pltpu.CompilerParams(vmem_limit_bytes=20 * 2**20),
    )(query_basis, output_basis, full, full, norm, query_weight, output_weight, mom, mom)


def solution(mesh):
    small = dict(mesh.shape) == {"fs": 4, "rep": 4, "tp": 2}
    body = on_device_fast if small else on_device
    placed = (
        P(("fs", "rep"), None),
        P(("fs", "rep"), "tp"),
        P(("fs", "rep"), "tp"),
        P(("fs", "rep"), None),
        P("fs", None),
        P("fs", None),
        P("fs", "tp"),
        P("tp", "fs"),
        P("rep", "tp"),
        P("tp", "rep"),
    )
    return jax.shard_map(
        body,
        mesh=mesh,
        in_specs=placed,
        out_specs=(
            P("fs", "tp"),
            P("tp", "fs"),
            P("fs", "tp"),
            P("tp", "fs"),
            P("fs", "tp"),
            P("tp", "fs"),
            P("rep", "tp"),
            P("tp", "rep"),
        ),
        check_vma=False,
    )
```
